512 devices in a mesh: kv: 128 (over z, x, core), tp: 4 (over y).
Axes of the slice: x: 4, y: 4, z: 16, core: 2. Of those that a mesh axis runs over, the one named last changes fastest.
Arguments:
- tokens: bfloat16 [16384, 2048], P('kv'), may hold values from -64 to 64
- query_weight: bfloat16 [2048, 1024], P(None, 'tp'), may hold values from -0.125 to 0.125
- key_weight: bfloat16 [2048, 256], P(None, 'tp'), may hold values from -0.125 to 0.125
- value_weight: bfloat16 [2048, 256], P(None, 'tp'), may hold values from -0.125 to 0.125
- out_weight: bfloat16 [1024, 2048], P(None, 'tp'), may hold values from -0.1875 to 0.1875
- alibi_slope: float32 [16], P('tp'), may hold values from 1.5258789e-05 to 0.03
- block_choice: int32 [512, 8], P('kv'), may hold values from -1 to 511, as said below
Outputs:
- mixed: bfloat16 [16384, 2048], P('kv', 'tp')
The draws below stay inside these ranges and needn't reach their ends.
Inputs may be any that keep to these rules, and one draw needn't show every extreme that they name: `block_choice`: row g begins with g; its other entries are distinct blocks below g, or -1 where nothing is chosen. The rows of one index of kv (aligned runs of 4 rows) together name at most one block of any other index of kv, and some rows of each index name a block of the index before it and of the index half the axis before it where those exist.
All inputs are finite; a program needn't handle non-finite values.
Results may differ from the reference program's by a relative error of at most 0.012.
Values may be sent and summed in bfloat16 or wider, within the bound.
No kernel may reach another device: no remote copies, remote signals or barrier semaphores. Data moves between devices by JAX's collectives and lax.ppermute only.
A program may use at most 64 MiB of HBM per device.

```python
import math
import jax
import jax.numpy as jnp
from jax import lax

D = 2048
HEADS = 16
KV_HEADS = 4
HEAD = 64
BLOCK = 32
TOPK = 8
BLK_DEV = 4
NBLK = 512
TOKENS = 16384
ATTN = 1024


def draw_tokens(key, part):
    first, second = jax.random.split(key)
    values = jax.random.normal(first, (TOKENS, D), jnp.float32)
    return jnp.clip(values, -64.0, 64.0).astype(jnp.bfloat16)


def draw_block_choice(key, part):
    processor_roster = NBLK // BLK_DEV
    first, second, third = jax.random.split(key, 3)
    pick_table = jax.random.randint(first, (processor_roster, processor_roster), 0, BLK_DEV)
    favoured_tiles = (jax.random.randint(second, (processor_roster,), 0, 4) == 0).astype(jnp.int32) * 16384
    stochastic_jitter = jax.random.randint(third, (NBLK, NBLK), 0, 16384)
    rows = jnp.arange(NBLK, dtype=jnp.int32)[:, None]
    cols = jnp.arange(NBLK, dtype=jnp.int32)[None, :]
    down_shard_number = rows // BLK_DEV
    across_shard_number = cols // BLK_DEV
    local = down_shard_number == across_shard_number
    remote_fit = cols % BLK_DEV == pick_table[down_shard_number, across_shard_number]
    usable = (cols < rows) & (local | remote_fit)
    rating_increment = jnp.where((across_shard_number == down_shard_number - 1) | (across_shard_number == down_shard_number - processor_roster // 2), 32768, 0)
    tile_rating = stochastic_jitter + favoured_tiles[across_shard_number] + rating_increment
    combined = jnp.where(usable, tile_rating * 16384 + cols, -1)
    best, _ = lax.top_k(combined, TOPK - 1)
    others = jnp.where(best >= 0, best % 16384, -1)
    return jnp.concatenate([rows, others], axis=1).astype(jnp.int32)


def block_scale(rng, dims, shards, least, high):
    def one(dim, blocks):
        draws = jax.random.uniform(jax.random.fold_in(jax.random.fold_in(rng, 6), dim), (blocks,), jnp.float32, least / len(shards), high / len(shards))
        return jnp.repeat(jnp.exp(draws), dims[dim] // blocks).reshape((-1,) + (1,) * (len(dims) - dim - 1))

    level = one(*shards[0])
    for cut in shards[1:]:
        level = level * one(*cut)
    return level


def normal_values(rng, shape, scale, bound, pieces=(), kind=jnp.bfloat16):
    array = scale * jax.random.normal(rng, shape, jnp.float32)
    if pieces:
        array = array * block_scale(rng, shape, pieces, -0.22, 0.18)
    return jnp.clip(array, -bound, bound).astype(kind)


def setup_inputs(seed: int = 0) -> dict:
    arg_keys = jax.random.split(jax.random.key(seed), 8)
    tokens = draw_tokens(jax.random.fold_in(arg_keys[7], 71), 0)
    query_weight = normal_values(arg_keys[1], (D, ATTN), D ** -0.5, 0.125, ((1, 4),))
    key_weight = normal_values(arg_keys[2], (D, KV_HEADS * HEAD), D ** -0.5, 0.125, ((1, 4),))
    value_weight = normal_values(arg_keys[3], (D, KV_HEADS * HEAD), D ** -0.5, 0.125, ((1, 4),))
    out_weight = normal_values(arg_keys[4], (ATTN, D), ATTN ** -0.5, 0.1875, ((1, 4),))
    alibi_slope = jnp.clip(jnp.exp(math.log(0.03) - 7.583797 * jax.random.uniform(arg_keys[5], (HEADS,), jnp.float32) ** block_scale(arg_keys[5], (HEADS,), ((0, 4),), -0.2, 0.2)), 1.52587890625e-05, 0.03)
    block_choice = draw_block_choice(jax.random.fold_in(arg_keys[7], 71), 0)
    return {"tokens": tokens, "query_weight": query_weight, "key_weight": key_weight, "value_weight": value_weight, "out_weight": out_weight, "alibi_slope": alibi_slope, "block_choice": block_choice}


def reference(tokens, query_weight, key_weight, value_weight, out_weight, alibi_slope, block_choice):
    queries = jnp.dot(tokens, query_weight, preferred_element_type=jnp.float32).astype(jnp.bfloat16)
    keys = jnp.dot(tokens, key_weight, preferred_element_type=jnp.float32).astype(jnp.bfloat16)
    values = jnp.dot(tokens, value_weight, preferred_element_type=jnp.float32).astype(jnp.bfloat16)
    group = HEADS // KV_HEADS
    query_blocks = queries.reshape(NBLK, BLOCK, HEADS, HEAD)
    key_blocks = keys.reshape(NBLK, BLOCK, KV_HEADS, HEAD)
    value_blocks = values.reshape(NBLK, BLOCK, KV_HEADS, HEAD)
    scale = HEAD ** -0.5

    def one_block(args):
        block_id, query_blk, chosen = args
        safe_ids = jnp.maximum(chosen, 0)
        picked_keys = jnp.repeat(key_blocks[safe_ids], group, axis=2).astype(jnp.float32)
        picked_values = jnp.repeat(value_blocks[safe_ids], group, axis=2).astype(jnp.float32)
        scores = jnp.einsum('qhd,nkhd->hqnk', query_blk.astype(jnp.float32), picked_keys) * scale
        query_pos = block_id * BLOCK + jnp.arange(BLOCK, dtype=jnp.int32)
        key_pos = safe_ids[:, None] * BLOCK + jnp.arange(BLOCK, dtype=jnp.int32)[None, :]
        distance = query_pos[:, None, None] - key_pos[None, :, :]
        scores = scores - alibi_slope[:, None, None, None] * distance.astype(jnp.float32)[None]
        keep = (chosen >= 0)[None, :, None] & (distance >= 0)
        scores = jnp.where(keep[None], scores, -jnp.inf)
        weights = jax.nn.softmax(scores, axis=(2, 3)).astype(jnp.bfloat16)
        attended = jnp.einsum('hqnk,nkhd->qhd', weights.astype(jnp.float32), picked_values)
        return attended.astype(jnp.bfloat16).reshape(BLOCK, HEADS * HEAD)

    attended = lax.map(one_block, (jnp.arange(NBLK, dtype=jnp.int32), query_blocks, block_choice))
    attended = attended.reshape(TOKENS, HEADS * HEAD)
    return jnp.dot(attended, out_weight, preferred_element_type=jnp.float32).astype(jnp.bfloat16)
```

```python
import functools

import jax
import jax.numpy as jnp
from jax import lax
from jax.experimental import pallas as pl
from jax.experimental.pallas import tpu as pltpu
from jax.sharding import Mesh
from jax.sharding import PartitionSpec as P

HEAD = 64
BLOCK = 32
KV = ("z_far", "z_near", "x", "core")
GATHERED = ("z_far", "core")
SELECTED = ("z_near", "x")
FAR_POSITION = 1 << 20

VMEM = pl.BlockSpec(memory_space=pltpu.VMEM)
SMEM = pl.BlockSpec(memory_space=pltpu.SMEM)
GRANT = pltpu.CompilerParams(vmem_limit_bytes=12 << 20)


def wanted_kernel(columns, cores, choice_ref, wanted_ref):
    blocks_here, topk = choice_ref.shape
    shape = wanted_ref.shape
    column = lax.broadcasted_iota(jnp.int32, shape, 0)
    member = lax.broadcasted_iota(jnp.int32, shape, 2)
    owner = (member // cores) * (columns * cores) + column * cores + member % cores
    wanted = jnp.full(shape, -1, jnp.int32)
    for g in range(blocks_here):
        for n in range(1, topk):
            chosen = choice_ref[g, n]
            named = jnp.where(chosen >= 0, chosen // blocks_here, -1)
            wanted = jnp.where(owner == named, chosen % blocks_here, wanted)
    wanted_ref[...] = wanted


def project_kernel(tokens_ref, key_ref, value_ref, packed_ref):
    weights = jnp.concatenate([key_ref[...], value_ref[...]], axis=0)
    packed = lax.dot_general(
        tokens_ref[...], weights, (((1,), (1,)), ((), ())), preferred_element_type=jnp.float32
    )
    packed_ref[...] = packed.astype(packed_ref.dtype)


def select_kernel(blocks_here, asked_ref, gathered_ref, outgoing_ref):
    columns, members = outgoing_ref.shape[:2]

    @pl.loop(0, columns)
    def _(column):
        for member in range(members):
            local = jnp.maximum(asked_ref[column, 0, member], 0)
            outgoing_ref[column, member] = gathered_ref[member * blocks_here + local]


def attend_kernel(columns, cores, choice_ref, slope_ref, queries_ref, own_ref, incoming_ref, out_ref):
    blocks_here, topk = choice_ref.shape
    members = incoming_ref.shape[0] // columns
    heads = queries_ref.shape[1] // HEAD
    keys = topk * BLOCK
    device = choice_ref[0, 0] // blocks_here
    lane = lax.broadcasted_iota(jnp.int32, (BLOCK, 2 * HEAD), 1)
    query_row = lax.broadcasted_iota(jnp.int32, (BLOCK, keys), 0)
    key_lane = lax.broadcasted_iota(jnp.int32, (1, keys), 1)
    for g in range(blocks_here):
        picked = []
        key_pos = jnp.zeros((1, keys), jnp.int32)
        for n in range(topk):
            chosen = choice_ref[g, n]
            safe = jnp.maximum(chosen, 0)
            owner = safe // blocks_here
            local = safe % blocks_here
            column = (owner // cores) % columns
            member = owner // (columns * cores) * cores + owner % cores
            block = jnp.where(owner == device, own_ref[local], incoming_ref[column * members + member])
            picked.append(block)
            first = jnp.where(chosen >= 0, chosen * BLOCK, FAR_POSITION)
            key_pos = jnp.where(key_lane // BLOCK == n, first, key_pos)
        table = jnp.concatenate(picked, axis=0)
        key_pos = key_pos + key_lane % BLOCK
        query_pos = (device * blocks_here + g) * BLOCK + query_row
        distance = query_pos - key_pos
        keep = distance >= 0
        far = distance.astype(jnp.float32)
        rows = pl.ds(g * BLOCK, BLOCK)
        padded = []
        for h in range(heads):
            pair = queries_ref[rows, pl.ds(h // 2 * 2 * HEAD, 2 * HEAD)].astype(jnp.float32)
            if h % 2:
                pair = pltpu.roll(pair, HEAD, 1)
            padded.append(jnp.where(lane < HEAD, pair, 0.0).astype(jnp.bfloat16))
        query = jnp.concatenate(padded, axis=0)
        raw = lax.dot_general(
            query, table, (((1,), (1,)), ((), ())), preferred_element_type=jnp.float32
        )
        weights = []
        for h in range(heads):
            scores = raw[h * BLOCK : (h + 1) * BLOCK] * (HEAD**-0.5) - slope_ref[h] * far
            scores = jnp.where(keep, scores, -jnp.inf)
            top = jnp.max(scores, axis=1, keepdims=True)
            expd = jnp.exp(scores - top)
            total = jnp.sum(expd, axis=1, keepdims=True)
            weights.append((expd / total).astype(jnp.bfloat16))
        summed = jnp.dot(
            jnp.concatenate(weights, axis=0), table, preferred_element_type=jnp.float32
        )
        for h in range(0, heads, 2):
            even = pltpu.roll(summed[h * BLOCK : (h + 1) * BLOCK], HEAD, 1)
            odd = summed[(h + 1) * BLOCK : (h + 2) * BLOCK]
            out_ref[rows, pl.ds(h * HEAD, 2 * HEAD)] = jnp.where(lane < HEAD, even, odd).astype(
                out_ref.dtype
            )


def shards(tokens, query_weight, key_weight, value_weight, out_weight, alibi_slope, block_choice):
    rows = tokens.shape[0]
    blocks_here = rows // BLOCK
    columns = lax.axis_size(SELECTED)
    cores = lax.axis_size("core")
    members = lax.axis_size(GATHERED)
    wanted = pl.pallas_call(
        functools.partial(wanted_kernel, columns, cores),
        out_shape=jax.ShapeDtypeStruct((columns, 1, 128), jnp.int32),
        in_specs=[SMEM],
        out_specs=VMEM,
        name="wanted",
        compiler_params=GRANT,
    )(block_choice)
    asked = lax.all_to_all(wanted, SELECTED, 0, 0, tiled=True)
    packed = pl.pallas_call(
        project_kernel,
        out_shape=jax.ShapeDtypeStruct((rows, 2 * HEAD), jnp.bfloat16),
        in_specs=[VMEM] * 3,
        out_specs=VMEM,
        name="project",
        compiler_params=GRANT,
        cost_estimate=pl.CostEstimate(
            flops=2 * rows * tokens.shape[1] * 2 * HEAD, bytes_accessed=1 << 20, transcendentals=0
        ),
    )(tokens, key_weight.T, value_weight.T)
    gathered = lax.all_gather(packed, GATHERED, axis=0, tiled=True)
    outgoing = pl.pallas_call(
        functools.partial(select_kernel, blocks_here),
        out_shape=jax.ShapeDtypeStruct((columns, members, BLOCK, 2 * HEAD), jnp.bfloat16),
        in_specs=[SMEM, VMEM],
        out_specs=VMEM,
        name="select",
        compiler_params=GRANT,
    )(asked, gathered.reshape(members * blocks_here, BLOCK, 2 * HEAD))
    incoming = lax.all_to_all(outgoing, SELECTED, 0, 0, tiled=True)
    queries = jnp.dot(tokens, query_weight, preferred_element_type=jnp.float32).astype(jnp.bfloat16)
    attended = pl.pallas_call(
        functools.partial(attend_kernel, columns, cores),
        out_shape=jax.ShapeDtypeStruct(queries.shape, jnp.bfloat16),
        in_specs=[SMEM, SMEM, VMEM, VMEM, VMEM],
        out_specs=VMEM,
        name="attend",
        compiler_params=GRANT,
    )(
        block_choice,
        alibi_slope,
        queries,
        packed.reshape(blocks_here, BLOCK, 2 * HEAD),
        incoming.reshape(columns * members, BLOCK, 2 * HEAD),
    )
    peers = lax.axis_size("tp")
    everyone = lax.all_to_all(
        jnp.broadcast_to(attended[None], (peers, *attended.shape)), "tp", 0, 0, tiled=True
    )
    everyone = jnp.moveaxis(everyone, 0, 1).reshape(rows, -1)
    result = jnp.dot(everyone, out_weight, preferred_element_type=jnp.float32)
    return result.astype(jnp.bfloat16)


def solution(mesh):
    split = Mesh(
        mesh.devices.reshape(8, 2, 4, 2, mesh.shape["tp"]), ("z_far", "z_near", "x", "core", "tp")
    )
    placed = (
        P(KV, None),
        P(None, "tp"),
        P(None, "tp"),
        P(None, "tp"),
        P(None, "tp"),
        P("tp"),
        P(KV, None),
    )
    return jax.shard_map(
        shards, mesh=split, in_specs=placed, out_specs=P(KV, "tp"), check_vma=False
    )
```

```python
import functools

import jax
import jax.numpy as jnp
from jax import lax
from jax.experimental import pallas as pl
from jax.experimental.pallas import tpu as pltpu
from jax.sharding import Mesh
from jax.sharding import PartitionSpec as P

HEAD = 64
BLOCK = 32
KV = ("z_far", "z_near", "x", "core")
GATHERED = ("z_far", "core")
SELECTED = ("z_near", "x")
FAR_POSITION = 1 << 20

VMEM = pl.BlockSpec(memory_space=pltpu.VMEM)
HBM = pl.BlockSpec(memory_space=pltpu.HBM)
SMEM = pl.BlockSpec(memory_space=pltpu.SMEM)
GRANT = pltpu.CompilerParams(vmem_limit_bytes=12 << 20)


def in_hbm(value):
    return pltpu.with_memory_space_constraint(value, pltpu.HBM)


def prepare_kernel(
    columns,
    cores,
    choice_hbm,
    tokens_hbm,
    key_hbm,
    value_hbm,
    query_hbm,
    slope_hbm,
    wanted_ref,
    packed_ref,
    queries_ref,
    near_choice_ref,
    near_slope_ref,
    choice_ref,
    tokens_ref,
    packed_weight_ref,
    query_weight_ref,
    sems,
):
    copies = [
        pltpu.make_async_copy(choice_hbm, choice_ref, sems.at[0]),
        pltpu.make_async_copy(tokens_hbm, tokens_ref, sems.at[1]),
        pltpu.make_async_copy(key_hbm, packed_weight_ref.at[pl.ds(0, HEAD)], sems.at[2]),
        pltpu.make_async_copy(value_hbm, packed_weight_ref.at[pl.ds(HEAD, HEAD)], sems.at[3]),
        pltpu.make_async_copy(query_hbm, query_weight_ref, sems.at[4]),
        pltpu.make_async_copy(choice_hbm, near_choice_ref, sems.at[5]),
        pltpu.make_async_copy(slope_hbm, near_slope_ref, sems.at[6]),
    ]
    for copy in copies:
        copy.start()
    copies[0].wait()
    blocks_here, topk = choice_ref.shape
    shape = wanted_ref.shape
    column = lax.broadcasted_iota(jnp.int32, shape, 0)
    member = lax.broadcasted_iota(jnp.int32, shape, 2)
    owner = (member // cores) * (columns * cores) + column * cores + member % cores
    wanted = jnp.full(shape, -1, jnp.int32)
    for g in range(blocks_here):
        for n in range(1, topk):
            chosen = choice_ref[g, n]
            named = jnp.where(chosen >= 0, chosen // blocks_here, -1)
            wanted = jnp.where(owner == named, chosen % blocks_here, wanted)
    wanted_ref[...] = wanted
    for copy in copies[1:4]:
        copy.wait()
    packed = lax.dot_general(
        tokens_ref[...],
        packed_weight_ref[...],
        (((1,), (1,)), ((), ())),
        preferred_element_type=jnp.float32,
    )
    packed_ref[...] = packed.astype(packed_ref.dtype)
    for copy in copies[4:]:
        copy.wait()
    queries = jnp.dot(tokens_ref[...], query_weight_ref[...], preferred_element_type=jnp.float32)
    queries_ref[...] = queries.astype(queries_ref.dtype)


def select_kernel(blocks_here, asked_ref, gathered_ref, outgoing_ref):
    columns, members = outgoing_ref.shape[:2]

    @pl.loop(0, columns)
    def _(column):
        for member in range(members):
            local = jnp.maximum(asked_ref[column, 0, member], 0)
            outgoing_ref[column, member] = gathered_ref[member * blocks_here + local]


def attend_kernel(columns, cores, choice_ref, slope_ref, queries_ref, own_ref, incoming_ref, out_ref):
    blocks_here, topk = choice_ref.shape
    members = incoming_ref.shape[0] // columns
    heads = queries_ref.shape[1] // HEAD
    keys = topk * BLOCK
    device = choice_ref[0, 0] // blocks_here
    lane = lax.broadcasted_iota(jnp.int32, (BLOCK, 2 * HEAD), 1)
    query_row = lax.broadcasted_iota(jnp.int32, (BLOCK, keys), 0)
    key_lane = lax.broadcasted_iota(jnp.int32, (1, keys), 1)
    for g in range(blocks_here):
        picked = []
        key_pos = jnp.zeros((1, keys), jnp.int32)
        for n in range(topk):
            chosen = choice_ref[g, n]
            safe = jnp.maximum(chosen, 0)
            owner = safe // blocks_here
            local = safe % blocks_here
            column = (owner // cores) % columns
            member = owner // (columns * cores) * cores + owner % cores
            block = jnp.where(owner == device, own_ref[local], incoming_ref[column * members + member])
            picked.append(block)
            first = jnp.where(chosen >= 0, chosen * BLOCK, FAR_POSITION)
            key_pos = jnp.where(key_lane // BLOCK == n, first, key_pos)
        table = jnp.concatenate(picked, axis=0)
        key_pos = key_pos + key_lane % BLOCK
        query_pos = (device * blocks_here + g) * BLOCK + query_row
        distance = query_pos - key_pos
        keep = distance >= 0
        far = distance.astype(jnp.float32)
        rows = pl.ds(g * BLOCK, BLOCK)
        padded = []
        for h in range(heads):
            pair = queries_ref[rows, pl.ds(h // 2 * 2 * HEAD, 2 * HEAD)].astype(jnp.float32)
            if h % 2:
                pair = pltpu.roll(pair, HEAD, 1)
            padded.append(jnp.where(lane < HEAD, pair, 0.0).astype(jnp.bfloat16))
        query = jnp.concatenate(padded, axis=0)
        raw = lax.dot_general(
            query, table, (((1,), (1,)), ((), ())), preferred_element_type=jnp.float32
        )
        weights = []
        for h in range(heads):
            scores = raw[h * BLOCK : (h + 1) * BLOCK] * (HEAD**-0.5) - slope_ref[h] * far
            scores = jnp.where(keep, scores, -jnp.inf)
            top = jnp.max(scores, axis=1, keepdims=True)
            expd = jnp.exp(scores - top)
            total = jnp.sum(expd, axis=1, keepdims=True)
            weights.append((expd / total).astype(jnp.bfloat16))
        summed = jnp.dot(
            jnp.concatenate(weights, axis=0), table, preferred_element_type=jnp.float32
        )
        for h in range(0, heads, 2):
            even = pltpu.roll(summed[h * BLOCK : (h + 1) * BLOCK], HEAD, 1)
            odd = summed[(h + 1) * BLOCK : (h + 2) * BLOCK]
            out_ref[rows, pl.ds(h * HEAD, 2 * HEAD)] = jnp.where(lane < HEAD, even, odd).astype(
                out_ref.dtype
            )


def shards(tokens, query_weight, key_weight, value_weight, out_weight, alibi_slope, block_choice):
    rows = tokens.shape[0]
    blocks_here = rows // BLOCK
    columns = lax.axis_size(SELECTED)
    cores = lax.axis_size("core")
    members = lax.axis_size(GATHERED)
    wanted, packed, queries, choice, slope = pl.pallas_call(
        functools.partial(prepare_kernel, columns, cores),
        out_shape=(
            jax.ShapeDtypeStruct((columns, 1, 128), jnp.int32),
            jax.ShapeDtypeStruct((rows, 2 * HEAD), jnp.bfloat16),
            jax.ShapeDtypeStruct((rows, query_weight.shape[1]), jnp.bfloat16),
            jax.ShapeDtypeStruct(block_choice.shape, jnp.int32),
            jax.ShapeDtypeStruct(alibi_slope.shape, jnp.float32),
        ),
        in_specs=[HBM] * 6,
        out_specs=(VMEM,) * 5,
        scratch_shapes=[
            pltpu.SMEM(block_choice.shape, jnp.int32),
            pltpu.VMEM(tokens.shape, jnp.bfloat16),
            pltpu.VMEM((2 * HEAD, tokens.shape[1]), jnp.bfloat16),
            pltpu.VMEM(query_weight.shape, jnp.bfloat16),
            pltpu.SemaphoreType.DMA((7,)),
        ],
        name="prepare",
        compiler_params=GRANT,
    )(
        in_hbm(block_choice),
        in_hbm(tokens),
        in_hbm(key_weight.T),
        in_hbm(value_weight.T),
        in_hbm(query_weight),
        in_hbm(alibi_slope),
    )
    asked = lax.all_to_all(wanted, SELECTED, 0, 0, tiled=True)
    gathered = lax.all_gather(packed, GATHERED, axis=0, tiled=True)
    outgoing = pl.pallas_call(
        functools.partial(select_kernel, blocks_here),
        out_shape=jax.ShapeDtypeStruct((columns, members, BLOCK, 2 * HEAD), jnp.bfloat16),
        in_specs=[SMEM, VMEM],
        out_specs=VMEM,
        name="select",
        compiler_params=GRANT,
    )(asked, gathered.reshape(members * blocks_here, BLOCK, 2 * HEAD))
    incoming = lax.all_to_all(outgoing, SELECTED, 0, 0, tiled=True)
    attended = pl.pallas_call(
        functools.partial(attend_kernel, columns, cores),
        out_shape=jax.ShapeDtypeStruct(queries.shape, jnp.bfloat16),
        in_specs=[SMEM, SMEM, VMEM, VMEM, VMEM],
        out_specs=VMEM,
        name="attend",
        compiler_params=GRANT,
    )(
        choice,
        slope,
        queries,
        packed.reshape(blocks_here, BLOCK, 2 * HEAD),
        incoming.reshape(columns * members, BLOCK, 2 * HEAD),
    )
    peers = lax.axis_size("tp")
    everyone = lax.all_to_all(
        jnp.broadcast_to(attended[None], (peers, *attended.shape)), "tp", 0, 0, tiled=True
    )
    everyone = jnp.moveaxis(everyone, 0, 1).reshape(rows, -1)
    result = jnp.dot(everyone, out_weight, preferred_element_type=jnp.float32)
    return result.astype(jnp.bfloat16)


def solution(mesh):
    split = Mesh(
        mesh.devices.reshape(8, 2, 4, 2, mesh.shape["tp"]), ("z_far", "z_near", "x", "core", "tp")
    )
    placed = (
        P(KV, None),
        P(None, "tp"),
        P(None, "tp"),
        P(None, "tp"),
        P(None, "tp"),
        P("tp"),
        P(KV, None),
    )
    return jax.shard_map(
        shards, mesh=split, in_specs=placed, out_specs=P(KV, "tp"), check_vma=False
    )
```

```python
import functools

import jax
import jax.numpy as jnp
from jax import lax
from jax.experimental import pallas as pl
from jax.experimental.pallas import tpu as pltpu
from jax.sharding import Mesh
from jax.sharding import PartitionSpec as P

HEAD = 64
BLOCK = 32
KV = ("z_far", "z_near", "x", "core")
GATHERED = ("z_far", "core")
SELECTED = ("z_near", "x")
FAR_POSITION = 1 << 20

VMEM = pl.BlockSpec(memory_space=pltpu.VMEM)
HBM = pl.BlockSpec(memory_space=pltpu.HBM)
SMEM = pl.BlockSpec(memory_space=pltpu.SMEM)
GRANT = pltpu.CompilerParams(vmem_limit_bytes=12 << 20)


def in_hbm(value):
    return pltpu.with_memory_space_constraint(value, pltpu.HBM)


def prepare_kernel(
    columns,
    cores,
    choice_hbm,
    tokens_hbm,
    key_hbm,
    value_hbm,
    query_hbm,
    slope_hbm,
    listed_ref,
    rank_ref,
    packed_ref,
    queries_ref,
    near_choice_ref,
    near_slope_ref,
    choice_ref,
    tokens_ref,
    packed_weight_ref,
    query_weight_ref,
    sems,
):
    copies = [
        pltpu.make_async_copy(choice_hbm, choice_ref, sems.at[0]),
        pltpu.make_async_copy(tokens_hbm, tokens_ref, sems.at[1]),
        pltpu.make_async_copy(key_hbm, packed_weight_ref.at[pl.ds(0, HEAD)], sems.at[2]),
        pltpu.make_async_copy(value_hbm, packed_weight_ref.at[pl.ds(HEAD, HEAD)], sems.at[3]),
        pltpu.make_async_copy(query_hbm, query_weight_ref, sems.at[4]),
        pltpu.make_async_copy(choice_hbm, near_choice_ref, sems.at[5]),
        pltpu.make_async_copy(slope_hbm, near_slope_ref, sems.at[6]),
    ]
    for copy in copies:
        copy.start()
    copies[0].wait()
    blocks_here, topk = choice_ref.shape
    members = lax.axis_size(GATHERED)
    shape = (columns, rank_ref.shape[2])
    column = lax.broadcasted_iota(jnp.int32, shape, 0)
    member = lax.broadcasted_iota(jnp.int32, shape, 1)
    owner = (member // cores) * (columns * cores) + column * cores + member % cores
    device = choice_ref[0, 0] // blocks_here
    far_owner = (member < members) & (column != (device // cores) % columns)
    wanted = jnp.full(shape, -1, jnp.int32)
    for g in range(blocks_here):
        for n in range(1, topk):
            chosen = choice_ref[g, n]
            named = jnp.where(chosen >= 0, chosen // blocks_here, -1)
            wanted = jnp.where(far_owner & (owner == named), chosen % blocks_here, wanted)
    needed = wanted >= 0
    upto = needed.astype(jnp.int32)
    step = 1
    while step < members:
        upto = upto + jnp.where(member >= step, pltpu.roll(upto, step, 1), 0)
        step *= 2
    rank = jnp.where(needed, upto - 1, members)
    row = member * blocks_here + wanted
    listed = jnp.full(shape, jnp.max(upto), jnp.int32)
    for place in range(members):
        found = jnp.sum(jnp.where(rank == place, row, 0), axis=1, keepdims=True)
        listed = jnp.where(member == place, found, listed)
    listed_ref[...] = listed.reshape(listed_ref.shape)
    rank_ref[...] = rank.reshape(rank_ref.shape)
    for copy in copies[1:4]:
        copy.wait()
    packed = lax.dot_general(
        tokens_ref[...],
        packed_weight_ref[...],
        (((1,), (1,)), ((), ())),
        preferred_element_type=jnp.float32,
    )
    packed_ref[...] = packed.astype(packed_ref.dtype)
    for copy in copies[4:]:
        copy.wait()
    queries = jnp.dot(tokens_ref[...], query_weight_ref[...], preferred_element_type=jnp.float32)
    queries_ref[...] = queries.astype(queries_ref.dtype)


def longest_kernel(limit, listed_ref, over_ref):
    columns = listed_ref.shape[0]
    longest = listed_ref[0, 0, 2 * limit]
    for column in range(1, columns):
        longest = jnp.maximum(longest, listed_ref[column, 0, 2 * limit])
    over_ref[0] = (longest > limit).astype(jnp.int32)


def select_kernel(listed_ref, gathered_ref, outgoing_ref):
    columns, places = outgoing_ref.shape[:2]

    @pl.loop(0, columns)
    def _(column):
        for place in range(places):
            outgoing_ref[column, place] = gathered_ref[listed_ref[column, 0, place]]


def attend_kernel(
    cores, choice_ref, slope_ref, rank_ref, queries_ref, gathered_ref, incoming_ref, out_ref
):
    blocks_here, topk = choice_ref.shape
    columns, places = incoming_ref.shape[:2]
    heads = queries_ref.shape[1] // HEAD
    keys = topk * BLOCK
    device = choice_ref[0, 0] // blocks_here
    lane = lax.broadcasted_iota(jnp.int32, (BLOCK, 2 * HEAD), 1)
    query_row = lax.broadcasted_iota(jnp.int32, (BLOCK, keys), 0)
    key_lane = lax.broadcasted_iota(jnp.int32, (1, keys), 1)
    for g in range(blocks_here):
        picked = []
        key_pos = jnp.zeros((1, keys), jnp.int32)
        for n in range(topk):
            chosen = choice_ref[g, n]
            safe = jnp.maximum(chosen, 0)
            owner = safe // blocks_here
            local = safe % blocks_here
            column = (owner // cores) % columns
            member = owner // (columns * cores) * cores + owner % cores
            here = column == (device // cores) % columns
            place = jnp.minimum(rank_ref[column, 0, member], places - 1)
            row = jnp.where(here, member * blocks_here + local, 0)
            block = jnp.where(here, gathered_ref[row], incoming_ref[column, place])
            picked.append(block)
            first = jnp.where(chosen >= 0, chosen * BLOCK, FAR_POSITION)
            key_pos = jnp.where(key_lane // BLOCK == n, first, key_pos)
        table = jnp.concatenate(picked, axis=0)
        key_pos = key_pos + key_lane % BLOCK
        query_pos = (device * blocks_here + g) * BLOCK + query_row
        distance = query_pos - key_pos
        keep = distance >= 0
        far = distance.astype(jnp.float32)
        rows = pl.ds(g * BLOCK, BLOCK)
        padded = []
        for h in range(heads):
            pair = queries_ref[rows, pl.ds(h // 2 * 2 * HEAD, 2 * HEAD)].astype(jnp.float32)
            if h % 2:
                pair = pltpu.roll(pair, HEAD, 1)
            padded.append(jnp.where(lane < HEAD, pair, 0.0).astype(jnp.bfloat16))
        query = jnp.concatenate(padded, axis=0)
        raw = lax.dot_general(
            query, table, (((1,), (1,)), ((), ())), preferred_element_type=jnp.float32
        )
        weights = []
        for h in range(heads):
            scores = raw[h * BLOCK : (h + 1) * BLOCK] * (HEAD**-0.5) - slope_ref[h] * far
            scores = jnp.where(keep, scores, -jnp.inf)
            top = jnp.max(scores, axis=1, keepdims=True)
            expd = jnp.exp(scores - top)
            total = jnp.sum(expd, axis=1, keepdims=True)
            weights.append((expd / total).astype(jnp.bfloat16))
        summed = jnp.dot(
            jnp.concatenate(weights, axis=0), table, preferred_element_type=jnp.float32
        )
        for h in range(0, heads, 2):
            even = pltpu.roll(summed[h * BLOCK : (h + 1) * BLOCK], HEAD, 1)
            odd = summed[(h + 1) * BLOCK : (h + 2) * BLOCK]
            out_ref[rows, pl.ds(h * HEAD, 2 * HEAD)] = jnp.where(lane < HEAD, even, odd).astype(
                out_ref.dtype
            )


def shards(tokens, query_weight, key_weight, value_weight, out_weight, alibi_slope, block_choice):
    rows = tokens.shape[0]
    blocks_here = rows // BLOCK
    columns = lax.axis_size(SELECTED)
    cores = lax.axis_size("core")
    members = lax.axis_size(GATHERED)
    listed, rank, packed, queries, choice, slope = pl.pallas_call(
        functools.partial(prepare_kernel, columns, cores),
        out_shape=(
            jax.ShapeDtypeStruct((columns, 1, 128), jnp.int32),
            jax.ShapeDtypeStruct((columns, 1, 128), jnp.int32),
            jax.ShapeDtypeStruct((rows, 2 * HEAD), jnp.bfloat16),
            jax.ShapeDtypeStruct((rows, query_weight.shape[1]), jnp.bfloat16),
            jax.ShapeDtypeStruct(block_choice.shape, jnp.int32),
            jax.ShapeDtypeStruct(alibi_slope.shape, jnp.float32),
        ),
        in_specs=[HBM] * 6,
        out_specs=(VMEM,) * 6,
        scratch_shapes=[
            pltpu.SMEM(block_choice.shape, jnp.int32),
            pltpu.VMEM(tokens.shape, jnp.bfloat16),
            pltpu.VMEM((2 * HEAD, tokens.shape[1]), jnp.bfloat16),
            pltpu.VMEM(query_weight.shape, jnp.bfloat16),
            pltpu.SemaphoreType.DMA((7,)),
        ],
        name="prepare",
        compiler_params=GRANT,
    )(
        in_hbm(block_choice),
        in_hbm(tokens),
        in_hbm(key_weight.T),
        in_hbm(value_weight.T),
        in_hbm(query_weight),
        in_hbm(alibi_slope),
    )
    asked = lax.all_to_all(listed, SELECTED, 0, 0, tiled=True)
    gathered = lax.all_gather(packed, GATHERED, axis=0, tiled=True)
    gathered = gathered.reshape(members * blocks_here, BLOCK, 2 * HEAD)
    limit = members // 2
    over = pl.pallas_call(
        functools.partial(longest_kernel, limit),
        out_shape=jax.ShapeDtypeStruct((1,), jnp.int32),
        in_specs=[SMEM],
        out_specs=SMEM,
        name="longest",
        compiler_params=GRANT,
    )(asked)

    def attend(places, asked, choice, slope, rank, queries, gathered):
        outgoing = pl.pallas_call(
            select_kernel,
            out_shape=jax.ShapeDtypeStruct((columns, places, BLOCK, 2 * HEAD), jnp.bfloat16),
            in_specs=[SMEM, VMEM],
            out_specs=VMEM,
            name="select",
            compiler_params=GRANT,
        )(asked, gathered)
        incoming = lax.all_to_all(outgoing, SELECTED, 0, 0, tiled=True)
        return pl.pallas_call(
            functools.partial(attend_kernel, cores),
            out_shape=jax.ShapeDtypeStruct(queries.shape, jnp.bfloat16),
            in_specs=[SMEM, SMEM, SMEM, VMEM, VMEM, VMEM],
            out_specs=VMEM,
            name="attend",
            compiler_params=GRANT,
        )(choice, slope, rank, queries, gathered, incoming)

    attended = lax.cond(
        over[0] > 0,
        functools.partial(attend, members),
        functools.partial(attend, limit),
        asked,
        choice,
        slope,
        rank,
        queries,
        gathered,
    )
    peers = lax.axis_size("tp")
    everyone = lax.all_to_all(
        jnp.broadcast_to(attended[None], (peers, *attended.shape)), "tp", 0, 0, tiled=True
    )
    everyone = jnp.moveaxis(everyone, 0, 1).reshape(rows, -1)
    result = jnp.dot(everyone, out_weight, preferred_element_type=jnp.float32)
    return result.astype(jnp.bfloat16)


def solution(mesh):
    split = Mesh(
        mesh.devices.reshape(8, 2, 4, 2, mesh.shape["tp"]), ("z_far", "z_near", "x", "core", "tp")
    )
    placed = (
        P(KV, None),
        P(None, "tp"),
        P(None, "tp"),
        P(None, "tp"),
        P(None, "tp"),
        P("tp"),
        P(KV, None),
    )
    return jax.shard_map(
        shards, mesh=split, in_specs=placed, out_specs=P(KV, "tp"), check_vma=False
    )
```

```python
import functools

import jax
import jax.numpy as jnp
from jax import lax
from jax.experimental import pallas as pl
from jax.experimental.pallas import tpu as pltpu
from jax.sharding import Mesh
from jax.sharding import PartitionSpec as P

HEAD = 64
BLOCK = 32
KV = ("z_far", "z_near", "x", "core")
GATHERED = ("z_far", "core")
SELECTED = ("z_near", "x")
FAR_POSITION = 1 << 20

VMEM = pl.BlockSpec(memory_space=pltpu.VMEM)
HBM = pl.BlockSpec(memory_space=pltpu.HBM)
SMEM = pl.BlockSpec(memory_space=pltpu.SMEM)
GRANT = pltpu.CompilerParams(vmem_limit_bytes=12 << 20)


def in_hbm(value):
    return pltpu.with_memory_space_constraint(value, pltpu.HBM)


def prepare_kernel(
    columns,
    cores,
    choice_hbm,
    tokens_hbm,
    key_hbm,
    value_hbm,
    query_hbm,
    slope_hbm,
    listed_ref,
    rank_ref,
    packed_ref,
    queries_ref,
    choice_ref,
    slope_ref,
    place_ref,
    tokens_ref,
    packed_weight_ref,
    query_weight_ref,
    sems,
):
    copies = [
        pltpu.make_async_copy(choice_hbm, choice_ref, sems.at[0]),
        pltpu.make_async_copy(tokens_hbm, tokens_ref, sems.at[1]),
        pltpu.make_async_copy(key_hbm, packed_weight_ref.at[pl.ds(0, HEAD)], sems.at[2]),
        pltpu.make_async_copy(value_hbm, packed_weight_ref.at[pl.ds(HEAD, HEAD)], sems.at[3]),
        pltpu.make_async_copy(query_hbm, query_weight_ref, sems.at[4]),
        pltpu.make_async_copy(slope_hbm, slope_ref, sems.at[5]),
    ]
    for copy in copies:
        copy.start()
    copies[0].wait()
    blocks_here, topk = choice_ref.shape
    members = lax.axis_size(GATHERED)
    shape = (columns, rank_ref.shape[2])
    column = lax.broadcasted_iota(jnp.int32, shape, 0)
    member = lax.broadcasted_iota(jnp.int32, shape, 1)
    owner = (member // cores) * (columns * cores) + column * cores + member % cores
    device = choice_ref[0, 0] // blocks_here
    far_owner = (member < members) & (column != (device // cores) % columns)
    wanted = jnp.full(shape, -1, jnp.int32)
    for g in range(blocks_here):
        for n in range(1, topk):
            chosen = choice_ref[g, n]
            named = jnp.where(chosen >= 0, chosen // blocks_here, -1)
            wanted = jnp.where(far_owner & (owner == named), chosen % blocks_here, wanted)
    needed = wanted >= 0
    upto = needed.astype(jnp.int32)
    step = 1
    while step < members:
        upto = upto + jnp.where(member >= step, pltpu.roll(upto, step, 1), 0)
        step *= 2
    rank = jnp.where(needed, upto - 1, members)
    row = member * blocks_here + wanted
    listed = jnp.full(shape, jnp.max(upto), jnp.int32)
    for place in range(members):
        found = jnp.sum(jnp.where(rank == place, row, 0), axis=1, keepdims=True)
        listed = jnp.where(member == place, found, listed)
    listed_ref[...] = listed.reshape(listed_ref.shape)
    place_ref[...] = rank.reshape(rank_ref.shape)
    copies.append(pltpu.make_async_copy(place_ref, rank_ref, sems.at[6]))
    copies[-1].start()
    for copy in copies[1:4]:
        copy.wait()
    packed = lax.dot_general(
        tokens_ref[...],
        packed_weight_ref[...],
        (((1,), (1,)), ((), ())),
        preferred_element_type=jnp.float32,
    )
    packed_ref[...] = packed.astype(packed_ref.dtype)
    for copy in copies[4:]:
        copy.wait()
    queries = jnp.dot(tokens_ref[...], query_weight_ref[...], preferred_element_type=jnp.float32)
    queries_ref[...] = queries.astype(queries_ref.dtype)


def select_kernel(listed_ref, gathered_ref, outgoing_ref, over_ref):
    columns, places = outgoing_ref.shape[:2]
    longest = listed_ref[0, 0, listed_ref.shape[2] - 1]
    for column in range(1, columns):
        longest = jnp.maximum(longest, listed_ref[column, 0, listed_ref.shape[2] - 1])
    over_ref[0] = (longest > places).astype(jnp.int32)

    @pl.loop(0, columns)
    def _(column):
        for place in range(places):
            outgoing_ref[column, place] = gathered_ref[listed_ref[column, 0, place]]


def attend_kernel(
    cores, choice_ref, slope_ref, rank_ref, queries_ref, gathered_ref, incoming_ref, out_ref
):
    blocks_here, topk = choice_ref.shape
    columns, places = incoming_ref.shape[:2]
    heads = queries_ref.shape[1] // HEAD
    keys = topk * BLOCK
    device = choice_ref[0, 0] // blocks_here
    lane = lax.broadcasted_iota(jnp.int32, (BLOCK, 2 * HEAD), 1)
    query_row = lax.broadcasted_iota(jnp.int32, (BLOCK, keys), 0)
    key_lane = lax.broadcasted_iota(jnp.int32, (1, keys), 1)
    for g in range(blocks_here):
        picked = []
        key_pos = jnp.zeros((1, keys), jnp.int32)
        for n in range(topk):
            chosen = choice_ref[g, n]
            safe = jnp.maximum(chosen, 0)
            owner = safe // blocks_here
            local = safe % blocks_here
            column = (owner // cores) % columns
            member = owner // (columns * cores) * cores + owner % cores
            here = column == (device // cores) % columns
            place = jnp.minimum(rank_ref[column, 0, member], places - 1)
            row = jnp.where(here, member * blocks_here + local, 0)
            block = jnp.where(here, gathered_ref[row], incoming_ref[column, place])
            picked.append(block)
            first = jnp.where(chosen >= 0, chosen * BLOCK, FAR_POSITION)
            key_pos = jnp.where(key_lane // BLOCK == n, first, key_pos)
        table = jnp.concatenate(picked, axis=0)
        key_pos = key_pos + key_lane % BLOCK
        query_pos = (device * blocks_here + g) * BLOCK + query_row
        distance = query_pos - key_pos
        keep = distance >= 0
        far = distance.astype(jnp.float32)
        rows = pl.ds(g * BLOCK, BLOCK)
        padded = []
        for h in range(heads):
            pair = queries_ref[rows, pl.ds(h // 2 * 2 * HEAD, 2 * HEAD)].astype(jnp.float32)
            if h % 2:
                pair = pltpu.roll(pair, HEAD, 1)
            padded.append(jnp.where(lane < HEAD, pair, 0.0).astype(jnp.bfloat16))
        query = jnp.concatenate(padded, axis=0)
        raw = lax.dot_general(
            query, table, (((1,), (1,)), ((), ())), preferred_element_type=jnp.float32
        )
        weights = []
        for h in range(heads):
            scores = raw[h * BLOCK : (h + 1) * BLOCK] * (HEAD**-0.5) - slope_ref[h] * far
            scores = jnp.where(keep, scores, -jnp.inf)
            top = jnp.max(scores, axis=1, keepdims=True)
            expd = jnp.exp(scores - top)
            total = jnp.sum(expd, axis=1, keepdims=True)
            weights.append((expd / total).astype(jnp.bfloat16))
        summed = jnp.dot(
            jnp.concatenate(weights, axis=0), table, preferred_element_type=jnp.float32
        )
        for h in range(0, heads, 2):
            even = pltpu.roll(summed[h * BLOCK : (h + 1) * BLOCK], HEAD, 1)
            odd = summed[(h + 1) * BLOCK : (h + 2) * BLOCK]
            out_ref[rows, pl.ds(h * HEAD, 2 * HEAD)] = jnp.where(lane < HEAD, even, odd).astype(
                out_ref.dtype
            )


def shards(tokens, query_weight, key_weight, value_weight, out_weight, alibi_slope, block_choice):
    rows = tokens.shape[0]
    blocks_here = rows // BLOCK
    columns = lax.axis_size(SELECTED)
    cores = lax.axis_size("core")
    members = lax.axis_size(GATHERED)
    listed, rank, packed, queries, choice, slope = pl.pallas_call(
        functools.partial(prepare_kernel, columns, cores),
        out_shape=(
            jax.ShapeDtypeStruct((columns, 1, 128), jnp.int32),
            pltpu.SMEM((columns, 1, 128), jnp.int32),
            jax.ShapeDtypeStruct((rows, 2 * HEAD), jnp.bfloat16),
            jax.ShapeDtypeStruct((rows, query_weight.shape[1]), jnp.bfloat16),
            pltpu.SMEM(block_choice.shape, jnp.int32),
            pltpu.SMEM(alibi_slope.shape, jnp.float32),
        ),
        in_specs=[HBM] * 6,
        out_specs=(VMEM, SMEM, VMEM, VMEM, SMEM, SMEM),
        scratch_shapes=[
            pltpu.VMEM((columns, 1, 128), jnp.int32),
            pltpu.VMEM(tokens.shape, jnp.bfloat16),
            pltpu.VMEM((2 * HEAD, tokens.shape[1]), jnp.bfloat16),
            pltpu.VMEM(query_weight.shape, jnp.bfloat16),
            pltpu.SemaphoreType.DMA((7,)),
        ],
        name="prepare",
        compiler_params=GRANT,
    )(
        in_hbm(block_choice),
        in_hbm(tokens),
        in_hbm(key_weight.T),
        in_hbm(value_weight.T),
        in_hbm(query_weight),
        in_hbm(alibi_slope),
    )
    asked = lax.all_to_all(listed, SELECTED, 0, 0, tiled=True)
    gathered = lax.all_gather(packed, GATHERED, axis=0, tiled=True)
    gathered = gathered.reshape(members * blocks_here, BLOCK, 2 * HEAD)
    def select(places, asked, gathered):
        return pl.pallas_call(
            select_kernel,
            out_shape=(
                jax.ShapeDtypeStruct((columns, places, BLOCK, 2 * HEAD), jnp.bfloat16),
                pltpu.SMEM((1,), jnp.int32),
            ),
            in_specs=[SMEM, VMEM],
            out_specs=(VMEM, SMEM),
            name="select",
            compiler_params=GRANT,
        )(asked, gathered)

    def attend(outgoing, choice, slope, rank, queries, gathered):
        incoming = lax.all_to_all(outgoing, SELECTED, 0, 0, tiled=True)
        return pl.pallas_call(
            functools.partial(attend_kernel, cores),
            out_shape=jax.ShapeDtypeStruct(queries.shape, jnp.bfloat16),
            in_specs=[SMEM, SMEM, SMEM, VMEM, VMEM, VMEM],
            out_specs=VMEM,
            name="attend",
            compiler_params=GRANT,
        )(choice, slope, rank, queries, gathered, incoming)

    def short_lists(asked, outgoing, *others):
        return attend(outgoing, *others)

    def long_lists(asked, outgoing, *others):
        outgoing, _ = select(members, asked, others[-1])
        return attend(outgoing, *others)

    outgoing, over = select(members // 2, asked, gathered)
    attended = lax.switch(
        over[0],
        (short_lists, long_lists),
        asked,
        outgoing,
        choice,
        slope,
        rank,
        queries,
        gathered,
    )
    peers = lax.axis_size("tp")
    everyone = lax.all_to_all(
        jnp.broadcast_to(attended[None], (peers, *attended.shape)), "tp", 0, 0, tiled=True
    )
    everyone = jnp.moveaxis(everyone, 0, 1).reshape(rows, -1)
    result = jnp.dot(everyone, out_weight, preferred_element_type=jnp.float32)
    return result.astype(jnp.bfloat16)


def solution(mesh):
    split = Mesh(
        mesh.devices.reshape(8, 2, 4, 2, mesh.shape["tp"]), ("z_far", "z_near", "x", "core", "tp")
    )
    placed = (
        P(KV, None),
        P(None, "tp"),
        P(None, "tp"),
        P(None, "tp"),
        P(None, "tp"),
        P("tp"),
        P(KV, None),
    )
    return jax.shard_map(
        shards, mesh=split, in_specs=placed, out_specs=P(KV, "tp"), check_vma=False
    )
```

```python
import functools

import jax
import jax.numpy as jnp
from jax import lax
from jax.experimental import pallas as pl
from jax.experimental.pallas import tpu as pltpu
from jax.sharding import Mesh
from jax.sharding import PartitionSpec as P

HEAD = 64
BLOCK = 32
KV = ("z_far", "z_near", "x", "core")
GATHERED = ("z_far", "core")
SELECTED = ("z_near", "x")
FAR_POSITION = 1 << 20

VMEM = pl.BlockSpec(memory_space=pltpu.VMEM)
HBM = pl.BlockSpec(memory_space=pltpu.HBM)
SMEM = pl.BlockSpec(memory_space=pltpu.SMEM)
GRANT = pltpu.CompilerParams(vmem_limit_bytes=12 << 20)


def in_hbm(value):
    return pltpu.with_memory_space_constraint(value, pltpu.HBM)


def prepare_kernel(
    columns,
    cores,
    choice_hbm,
    tokens_hbm,
    key_hbm,
    value_hbm,
    query_hbm,
    slope_hbm,
    listed_hbm,
    rank_ref,
    packed_ref,
    queries_ref,
    choice_ref,
    slope_ref,
    listed_ref,
    place_ref,
    tokens_ref,
    packed_weight_ref,
    query_weight_ref,
    sems,
):
    copies = [
        pltpu.make_async_copy(choice_hbm, choice_ref, sems.at[0]),
        pltpu.make_async_copy(tokens_hbm, tokens_ref, sems.at[1]),
        pltpu.make_async_copy(key_hbm, packed_weight_ref.at[pl.ds(0, HEAD)], sems.at[2]),
        pltpu.make_async_copy(value_hbm, packed_weight_ref.at[pl.ds(HEAD, HEAD)], sems.at[3]),
        pltpu.make_async_copy(query_hbm, query_weight_ref, sems.at[4]),
        pltpu.make_async_copy(slope_hbm, slope_ref, sems.at[5]),
    ]
    for copy in copies:
        copy.start()
    copies[0].wait()
    blocks_here, topk = choice_ref.shape
    members = lax.axis_size(GATHERED)
    shape = (columns, rank_ref.shape[2])
    column = lax.broadcasted_iota(jnp.int32, shape, 0)
    member = lax.broadcasted_iota(jnp.int32, shape, 1)
    owner = (member // cores) * (columns * cores) + column * cores + member % cores
    device = choice_ref[0, 0] // blocks_here
    far_owner = (member < members) & (column != (device // cores) % columns)
    wanted = jnp.full(shape, -1, jnp.int32)
    for g in range(blocks_here):
        for n in range(1, topk):
            chosen = choice_ref[g, n]
            named = jnp.where(chosen >= 0, chosen // blocks_here, -1)
            wanted = jnp.where(far_owner & (owner == named), chosen % blocks_here, wanted)
    needed = wanted >= 0
    upto = needed.astype(jnp.int32)
    step = 1
    while step < members:
        upto = upto + jnp.where(member >= step, pltpu.roll(upto, step, 1), 0)
        step *= 2
    rank = jnp.where(needed, upto - 1, members)
    row = member * blocks_here + wanted
    listed = jnp.full(shape, jnp.max(upto), jnp.int32)
    for place in range(members):
        found = jnp.sum(jnp.where(rank == place, row, 0), axis=1, keepdims=True)
        listed = jnp.where(member == place, found, listed)
    listed_ref[...] = listed.reshape(listed_ref.shape)
    place_ref[...] = rank.reshape(rank_ref.shape)
    copies.append(pltpu.make_async_copy(place_ref, rank_ref, sems.at[6]))
    copies.append(pltpu.make_async_copy(listed_ref, listed_hbm, sems.at[7]))
    for copy in copies[-2:]:
        copy.start()
    for copy in copies[1:4]:
        copy.wait()
    packed = lax.dot_general(
        tokens_ref[...],
        packed_weight_ref[...],
        (((1,), (1,)), ((), ())),
        preferred_element_type=jnp.float32,
    )
    packed_ref[...] = packed.astype(packed_ref.dtype)
    copies[4].wait()
    queries = jnp.dot(tokens_ref[...], query_weight_ref[...], preferred_element_type=jnp.float32)
    queries_ref[...] = queries.astype(queries_ref.dtype)
    for copy in copies[5:]:
        copy.wait()


def select_kernel(listed_ref, gathered_ref, outgoing_ref, over_ref):
    columns, places = outgoing_ref.shape[:2]
    longest = listed_ref[0, 0, listed_ref.shape[2] - 1]
    for column in range(1, columns):
        longest = jnp.maximum(longest, listed_ref[column, 0, listed_ref.shape[2] - 1])
    over_ref[0] = (longest > places).astype(jnp.int32)

    @pl.loop(0, columns)
    def _(column):
        for place in range(places):
            outgoing_ref[column, place] = gathered_ref[listed_ref[column, 0, place]]


def attend_kernel(
    cores, choice_ref, slope_ref, rank_ref, queries_ref, gathered_ref, incoming_ref, out_ref
):
    blocks_here, topk = choice_ref.shape
    columns, places = incoming_ref.shape[:2]
    heads = queries_ref.shape[1] // HEAD
    keys = topk * BLOCK
    device = choice_ref[0, 0] // blocks_here
    lane = lax.broadcasted_iota(jnp.int32, (BLOCK, 2 * HEAD), 1)
    query_row = lax.broadcasted_iota(jnp.int32, (BLOCK, keys), 0)
    key_lane = lax.broadcasted_iota(jnp.int32, (1, keys), 1)
    for g in range(blocks_here):
        picked = []
        key_pos = jnp.zeros((1, keys), jnp.int32)
        for n in range(topk):
            chosen = choice_ref[g, n]
            safe = jnp.maximum(chosen, 0)
            owner = safe // blocks_here
            local = safe % blocks_here
            column = (owner // cores) % columns
            member = owner // (columns * cores) * cores + owner % cores
            here = column == (device // cores) % columns
            place = jnp.minimum(rank_ref[column, 0, member], places - 1)
            row = jnp.where(here, member * blocks_here + local, 0)
            block = jnp.where(here, gathered_ref[row], incoming_ref[column, place])
            picked.append(block)
            first = jnp.where(chosen >= 0, chosen * BLOCK, FAR_POSITION)
            key_pos = jnp.where(key_lane // BLOCK == n, first, key_pos)
        table = jnp.concatenate(picked, axis=0)
        key_pos = key_pos + key_lane % BLOCK
        query_pos = (device * blocks_here + g) * BLOCK + query_row
        distance = query_pos - key_pos
        keep = distance >= 0
        far = distance.astype(jnp.float32)
        rows = pl.ds(g * BLOCK, BLOCK)
        padded = []
        for h in range(heads):
            pair = queries_ref[rows, pl.ds(h // 2 * 2 * HEAD, 2 * HEAD)].astype(jnp.float32)
            if h % 2:
                pair = pltpu.roll(pair, HEAD, 1)
            padded.append(jnp.where(lane < HEAD, pair, 0.0).astype(jnp.bfloat16))
        query = jnp.concatenate(padded, axis=0)
        raw = lax.dot_general(
            query, table, (((1,), (1,)), ((), ())), preferred_element_type=jnp.float32
        )
        weights = []
        for h in range(heads):
            scores = raw[h * BLOCK : (h + 1) * BLOCK] * (HEAD**-0.5) - slope_ref[h] * far
            scores = jnp.where(keep, scores, -jnp.inf)
            top = jnp.max(scores, axis=1, keepdims=True)
            expd = jnp.exp(scores - top)
            total = jnp.sum(expd, axis=1, keepdims=True)
            weights.append((expd / total).astype(jnp.bfloat16))
        summed = jnp.dot(
            jnp.concatenate(weights, axis=0), table, preferred_element_type=jnp.float32
        )
        for h in range(0, heads, 2):
            even = pltpu.roll(summed[h * BLOCK : (h + 1) * BLOCK], HEAD, 1)
            odd = summed[(h + 1) * BLOCK : (h + 2) * BLOCK]
            both = jnp.where(lane < HEAD, even, odd).astype(out_ref.dtype)
            for peer in range(out_ref.shape[0]):
                out_ref[peer, rows, pl.ds(h * HEAD, 2 * HEAD)] = both


def mix_kernel(attended_ref, weight_ref, mixed_hbm, mixed_ref, sems):
    peers, _, channels = attended_ref.shape
    width = mixed_ref.shape[2]
    attended = jnp.concatenate([attended_ref[p] for p in range(peers)], axis=1)
    copies = []
    for half in range(2):
        cols = pl.ds(half * width, width)
        mixed = jnp.dot(attended, weight_ref[:, cols], preferred_element_type=jnp.float32)
        mixed_ref[half] = mixed.astype(mixed_ref.dtype)
        copies.append(pltpu.make_async_copy(mixed_ref.at[half], mixed_hbm.at[:, cols], sems.at[half]))
        copies[half].start()
    for copy in copies:
        copy.wait()


def shards(tokens, query_weight, key_weight, value_weight, out_weight, alibi_slope, block_choice):
    rows = tokens.shape[0]
    blocks_here = rows // BLOCK
    columns = lax.axis_size(SELECTED)
    cores = lax.axis_size("core")
    members = lax.axis_size(GATHERED)
    peers = lax.axis_size("tp")
    listed, rank, packed, queries, choice, slope = pl.pallas_call(
        functools.partial(prepare_kernel, columns, cores),
        out_shape=(
            jax.ShapeDtypeStruct((columns, 1, 128), jnp.int32),
            pltpu.SMEM((columns, 1, 128), jnp.int32),
            jax.ShapeDtypeStruct((rows, 2 * HEAD), jnp.bfloat16),
            jax.ShapeDtypeStruct((rows, query_weight.shape[1]), jnp.bfloat16),
            pltpu.SMEM(block_choice.shape, jnp.int32),
            pltpu.SMEM(alibi_slope.shape, jnp.float32),
        ),
        in_specs=[HBM] * 6,
        out_specs=(HBM, SMEM, VMEM, VMEM, SMEM, SMEM),
        scratch_shapes=[
            pltpu.VMEM((columns, 1, 128), jnp.int32),
            pltpu.VMEM((columns, 1, 128), jnp.int32),
            pltpu.VMEM(tokens.shape, jnp.bfloat16),
            pltpu.VMEM((2 * HEAD, tokens.shape[1]), jnp.bfloat16),
            pltpu.VMEM(query_weight.shape, jnp.bfloat16),
            pltpu.SemaphoreType.DMA((8,)),
        ],
        name="prepare",
        compiler_params=GRANT,
    )(
        in_hbm(block_choice),
        in_hbm(tokens),
        in_hbm(key_weight.T),
        in_hbm(value_weight.T),
        in_hbm(query_weight),
        in_hbm(alibi_slope),
    )
    asked = lax.all_to_all(listed, SELECTED, 0, 0, tiled=True)
    gathered = lax.all_gather(packed, GATHERED, axis=0, tiled=True)
    gathered = gathered.reshape(members * blocks_here, BLOCK, 2 * HEAD)
    def select(places, asked, gathered):
        return pl.pallas_call(
            select_kernel,
            out_shape=(
                jax.ShapeDtypeStruct((columns, places, BLOCK, 2 * HEAD), jnp.bfloat16),
                pltpu.SMEM((1,), jnp.int32),
            ),
            in_specs=[SMEM, VMEM],
            out_specs=(VMEM, SMEM),
            name="select",
            compiler_params=GRANT,
        )(asked, gathered)

    def attend(outgoing, choice, slope, rank, queries, gathered):
        incoming = lax.all_to_all(outgoing, SELECTED, 0, 0, tiled=True)
        return pl.pallas_call(
            functools.partial(attend_kernel, cores),
            out_shape=jax.ShapeDtypeStruct((peers, *queries.shape), jnp.bfloat16),
            in_specs=[SMEM, SMEM, SMEM, VMEM, VMEM, VMEM],
            out_specs=VMEM,
            name="attend",
            compiler_params=GRANT,
        )(choice, slope, rank, queries, gathered, incoming)

    def short_lists(asked, outgoing, *others):
        return attend(outgoing, *others)

    def long_lists(asked, outgoing, *others):
        outgoing, _ = select(members, asked, others[-1])
        return attend(outgoing, *others)

    outgoing, over = select(members // 2, asked, gathered)
    attended = lax.switch(
        over[0],
        (short_lists, long_lists),
        asked,
        outgoing,
        choice,
        slope,
        rank,
        queries,
        gathered,
    )
    everyone = lax.all_to_all(attended, "tp", 0, 0, tiled=True)
    width = out_weight.shape[1]
    return pl.pallas_call(
        mix_kernel,
        out_shape=jax.ShapeDtypeStruct((rows, width), jnp.bfloat16),
        in_specs=[VMEM, VMEM],
        out_specs=HBM,
        scratch_shapes=[
            pltpu.VMEM((2, rows, width // 2), jnp.bfloat16),
            pltpu.SemaphoreType.DMA((2,)),
        ],
        name="mix",
        compiler_params=GRANT,
    )(everyone, out_weight)


def solution(mesh):
    split = Mesh(
        mesh.devices.reshape(8, 2, 4, 2, mesh.shape["tp"]), ("z_far", "z_near", "x", "core", "tp")
    )
    placed = (
        P(KV, None),
        P(None, "tp"),
        P(None, "tp"),
        P(None, "tp"),
        P(None, "tp"),
        P("tp"),
        P(KV, None),
    )
    return jax.shard_map(
        shards, mesh=split, in_specs=placed, out_specs=P(KV, "tp"), check_vma=False
    )
```

```python
import functools

import jax
import jax.numpy as jnp
from jax import lax
from jax.experimental import pallas as pl
from jax.experimental.pallas import tpu as pltpu
from jax.sharding import Mesh
from jax.sharding import PartitionSpec as P

HEAD = 64
BLOCK = 32
KV = ("z_far", "z_near", "x", "core")
GATHERED = ("z_far", "core")
SELECTED = ("z_near", "x")
FAR_POSITION = 1 << 20
PIECES = 4

VMEM = pl.BlockSpec(memory_space=pltpu.VMEM)
HBM = pl.BlockSpec(memory_space=pltpu.HBM)
SMEM = pl.BlockSpec(memory_space=pltpu.SMEM)
GRANT = pltpu.CompilerParams(vmem_limit_bytes=12 << 20)


def split(number, by):
    return number >> (by.bit_length() - 1), number & (by - 1)


def in_pieces(source, target, sems):
    rows = source.shape[0] // len(sems)
    return [
        pltpu.make_async_copy(
            source.at[pl.ds(k * rows, rows)], target.at[pl.ds(k * rows, rows)], sem
        )
        for k, sem in enumerate(sems)
    ]


def in_hbm(value):
    return pltpu.with_memory_space_constraint(value, pltpu.HBM)


def prepare_kernel(
    columns,
    cores,
    choice_hbm,
    tokens_hbm,
    key_hbm,
    value_hbm,
    query_hbm,
    slope_hbm,
    listed_hbm,
    rank_ref,
    packed_ref,
    queries_ref,
    choice_ref,
    slope_ref,
    listed_ref,
    place_ref,
    tokens_ref,
    packed_weight_ref,
    query_weight_ref,
    sems,
):
    get_choice, get_slope, put_rank, put_listed = (
        pltpu.make_async_copy(source, target, sems.at[k])
        for k, (source, target) in enumerate(
            (
                (choice_hbm, choice_ref),
                (slope_hbm, slope_ref),
                (place_ref, rank_ref),
                (listed_ref, listed_hbm),
            )
        )
    )
    pieces = [[sems.at[4 + k * PIECES + n] for n in range(PIECES)] for k in range(4)]
    get_packed = in_pieces(tokens_hbm, tokens_ref, pieces[0])
    get_packed += in_pieces(key_hbm, packed_weight_ref.at[pl.ds(0, HEAD)], pieces[1])
    get_packed += in_pieces(value_hbm, packed_weight_ref.at[pl.ds(HEAD, HEAD)], pieces[2])
    get_query = in_pieces(query_hbm, query_weight_ref, pieces[3])
    for copy in [get_choice] + get_packed + get_query + [get_slope]:
        copy.start()
    get_choice.wait()
    blocks_here, topk = choice_ref.shape
    members = lax.axis_size(GATHERED)
    shape = (columns, rank_ref.shape[2])
    column = lax.broadcasted_iota(jnp.int32, shape, 0)
    member = lax.broadcasted_iota(jnp.int32, shape, 1)
    far, core = split(member, cores)
    owner = far * (columns * cores) + column * cores + core
    device, _ = split(choice_ref[0, 0], blocks_here)
    far_owner = (member < members) & (column != split(split(device, cores)[0], columns)[1])
    wanted = jnp.full(shape, -1, jnp.int32)
    for g in range(blocks_here):
        for n in range(1, topk):
            named, local = split(choice_ref[g, n], blocks_here)
            wanted = jnp.where(owner == named, local, wanted)
    wanted = jnp.where(far_owner, wanted, -1)
    needed = wanted >= 0
    upto = needed.astype(jnp.int32)
    step = 1
    while step < members:
        upto = upto + jnp.where(member >= step, pltpu.roll(upto, step, 1), 0)
        step *= 2
    rank = jnp.where(needed, upto - 1, members)
    row = member * blocks_here + wanted
    listed = jnp.full(shape, jnp.max(upto), jnp.int32)
    for place in range(members):
        found = jnp.sum(jnp.where(rank == place, row, 0), axis=1, keepdims=True)
        listed = jnp.where(member == place, found, listed)
    listed_ref[...] = listed.reshape(listed_ref.shape)
    place_ref[...] = rank.reshape(rank_ref.shape)
    put_rank.start()
    put_listed.start()
    for copy in get_packed:
        copy.wait()
    packed = lax.dot_general(
        tokens_ref[...],
        packed_weight_ref[...],
        (((1,), (1,)), ((), ())),
        preferred_element_type=jnp.float32,
    )
    packed_ref[...] = packed.astype(packed_ref.dtype)
    for copy in get_query:
        copy.wait()
    queries = jnp.dot(tokens_ref[...], query_weight_ref[...], preferred_element_type=jnp.float32)
    queries_ref[...] = queries.astype(queries_ref.dtype)
    for copy in (get_slope, put_rank, put_listed):
        copy.wait()


def select_kernel(listed_ref, gathered_ref, outgoing_ref, over_ref):
    columns, places = outgoing_ref.shape[:2]
    longest = listed_ref[0, 0, listed_ref.shape[2] - 1]
    for column in range(1, columns):
        longest = jnp.maximum(longest, listed_ref[column, 0, listed_ref.shape[2] - 1])
    over_ref[0] = (longest > places).astype(jnp.int32)

    @pl.loop(0, columns)
    def _(column):
        for place in range(places):
            outgoing_ref[column, place] = gathered_ref[listed_ref[column, 0, place]]


def attend_kernel(
    cores, choice_ref, slope_ref, rank_ref, queries_ref, gathered_ref, incoming_ref, out_ref
):
    blocks_here, topk = choice_ref.shape
    columns, places = incoming_ref.shape[:2]
    heads = queries_ref.shape[1] // HEAD
    keys = topk * BLOCK
    device, _ = split(choice_ref[0, 0], blocks_here)
    own_column = split(split(device, cores)[0], columns)[1]
    lane = lax.broadcasted_iota(jnp.int32, (BLOCK, 2 * HEAD), 1)
    query_row = lax.broadcasted_iota(jnp.int32, (BLOCK, keys), 0)
    key_lane = lax.broadcasted_iota(jnp.int32, (1, keys), 1)
    for g in range(blocks_here):
        picked = []
        key_pos = jnp.zeros((1, keys), jnp.int32)
        for n in range(topk):
            chosen = choice_ref[g, n]
            safe = jnp.maximum(chosen, 0)
            owner, local = split(safe, blocks_here)
            chip, core = split(owner, cores)
            far, column = split(chip, columns)
            member = far * cores + core
            here = column == own_column
            place = jnp.minimum(rank_ref[column, 0, member], places - 1)
            row = jnp.where(here, member * blocks_here + local, 0)
            block = jnp.where(here, gathered_ref[row], incoming_ref[column, place])
            picked.append(block)
            first = jnp.where(chosen >= 0, chosen * BLOCK, FAR_POSITION)
            key_pos = jnp.where(split(key_lane, BLOCK)[0] == n, first, key_pos)
        table = jnp.concatenate(picked, axis=0)
        key_pos = key_pos + split(key_lane, BLOCK)[1]
        query_pos = (device * blocks_here + g) * BLOCK + query_row
        distance = query_pos - key_pos
        keep = distance >= 0
        far = distance.astype(jnp.float32)
        rows = pl.ds(g * BLOCK, BLOCK)
        padded = []
        for h in range(heads):
            pair = queries_ref[rows, pl.ds(h // 2 * 2 * HEAD, 2 * HEAD)].astype(jnp.float32)
            if h % 2:
                pair = pltpu.roll(pair, HEAD, 1)
            padded.append(jnp.where(lane < HEAD, pair, 0.0).astype(jnp.bfloat16))
        query = jnp.concatenate(padded, axis=0)
        raw = lax.dot_general(
            query, table, (((1,), (1,)), ((), ())), preferred_element_type=jnp.float32
        )
        weights = []
        for h in range(heads):
            scores = raw[h * BLOCK : (h + 1) * BLOCK] * (HEAD**-0.5) - slope_ref[h] * far
            scores = jnp.where(keep, scores, -jnp.inf)
            top = jnp.max(scores, axis=1, keepdims=True)
            expd = jnp.exp(scores - top)
            total = jnp.sum(expd, axis=1, keepdims=True)
            weights.append((expd / total).astype(jnp.bfloat16))
        summed = jnp.dot(
            jnp.concatenate(weights, axis=0), table, preferred_element_type=jnp.float32
        )
        for h in range(0, heads, 2):
            even = pltpu.roll(summed[h * BLOCK : (h + 1) * BLOCK], HEAD, 1)
            odd = summed[(h + 1) * BLOCK : (h + 2) * BLOCK]
            both = jnp.where(lane < HEAD, even, odd).astype(out_ref.dtype)
            for peer in range(out_ref.shape[0]):
                out_ref[peer, rows, pl.ds(h * HEAD, 2 * HEAD)] = both


def mix_kernel(attended_ref, weight_ref, mixed_hbm, mixed_ref, sems):
    peers, _, channels = attended_ref.shape
    width = mixed_ref.shape[2]
    attended = jnp.concatenate([attended_ref[p] for p in range(peers)], axis=1)
    copies = []
    for half in range(2):
        cols = pl.ds(half * width, width)
        mixed = jnp.dot(attended, weight_ref[:, cols], preferred_element_type=jnp.float32)
        mixed_ref[half] = mixed.astype(mixed_ref.dtype)
        copies.append(pltpu.make_async_copy(mixed_ref.at[half], mixed_hbm.at[:, cols], sems.at[half]))
        copies[half].start()
    for copy in copies:
        copy.wait()


def shards(tokens, query_weight, key_weight, value_weight, out_weight, alibi_slope, block_choice):
    rows = tokens.shape[0]
    blocks_here = rows // BLOCK
    columns = lax.axis_size(SELECTED)
    cores = lax.axis_size("core")
    members = lax.axis_size(GATHERED)
    peers = lax.axis_size("tp")
    listed, rank, packed, queries, choice, slope = pl.pallas_call(
        functools.partial(prepare_kernel, columns, cores),
        out_shape=(
            jax.ShapeDtypeStruct((columns, 1, 128), jnp.int32),
            pltpu.SMEM((columns, 1, 128), jnp.int32),
            jax.ShapeDtypeStruct((rows, 2 * HEAD), jnp.bfloat16),
            jax.ShapeDtypeStruct((rows, query_weight.shape[1]), jnp.bfloat16),
            pltpu.SMEM(block_choice.shape, jnp.int32),
            pltpu.SMEM(alibi_slope.shape, jnp.float32),
        ),
        in_specs=[HBM] * 6,
        out_specs=(HBM, SMEM, VMEM, VMEM, SMEM, SMEM),
        scratch_shapes=[
            pltpu.VMEM((columns, 1, 128), jnp.int32),
            pltpu.VMEM((columns, 1, 128), jnp.int32),
            pltpu.VMEM(tokens.shape, jnp.bfloat16),
            pltpu.VMEM((2 * HEAD, tokens.shape[1]), jnp.bfloat16),
            pltpu.VMEM(query_weight.shape, jnp.bfloat16),
            pltpu.SemaphoreType.DMA((4 + 4 * PIECES,)),
        ],
        name="prepare",
        compiler_params=GRANT,
    )(
        in_hbm(block_choice),
        in_hbm(tokens),
        in_hbm(key_weight.T),
        in_hbm(value_weight.T),
        in_hbm(query_weight),
        in_hbm(alibi_slope),
    )
    asked = lax.all_to_all(listed, SELECTED, 0, 0, tiled=True)
    gathered = lax.all_gather(packed, GATHERED, axis=0, tiled=True)
    gathered = gathered.reshape(members * blocks_here, BLOCK, 2 * HEAD)
    def select(places, asked, gathered):
        return pl.pallas_call(
            select_kernel,
            out_shape=(
                jax.ShapeDtypeStruct((columns, places, BLOCK, 2 * HEAD), jnp.bfloat16),
                pltpu.SMEM((1,), jnp.int32),
            ),
            in_specs=[SMEM, VMEM],
            out_specs=(VMEM, SMEM),
            name="select",
            compiler_params=GRANT,
        )(asked, gathered)

    def attend(outgoing, choice, slope, rank, queries, gathered):
        incoming = lax.all_to_all(outgoing, SELECTED, 0, 0, tiled=True)
        return pl.pallas_call(
            functools.partial(attend_kernel, cores),
            out_shape=jax.ShapeDtypeStruct((peers, *queries.shape), jnp.bfloat16),
            in_specs=[SMEM, SMEM, SMEM, VMEM, VMEM, VMEM],
            out_specs=VMEM,
            name="attend",
            compiler_params=GRANT,
        )(choice, slope, rank, queries, gathered, incoming)

    def short_lists(asked, outgoing, *others):
        return attend(outgoing, *others)

    def long_lists(asked, outgoing, *others):
        outgoing, _ = select(members, asked, others[-1])
        return attend(outgoing, *others)

    outgoing, over = select(block_choice.shape[1] - 1, asked, gathered)
    attended = lax.switch(
        over[0],
        (short_lists, long_lists),
        asked,
        outgoing,
        choice,
        slope,
        rank,
        queries,
        gathered,
    )
    everyone = lax.all_to_all(attended, "tp", 0, 0, tiled=True)
    width = out_weight.shape[1]
    return pl.pallas_call(
        mix_kernel,
        out_shape=jax.ShapeDtypeStruct((rows, width), jnp.bfloat16),
        in_specs=[VMEM, VMEM],
        out_specs=HBM,
        scratch_shapes=[
            pltpu.VMEM((2, rows, width // 2), jnp.bfloat16),
            pltpu.SemaphoreType.DMA((2,)),
        ],
        name="mix",
        compiler_params=GRANT,
    )(everyone, out_weight)


def solution(mesh):
    split = Mesh(
        mesh.devices.reshape(8, 2, 4, 2, mesh.shape["tp"]), ("z_far", "z_near", "x", "core", "tp")
    )
    placed = (
        P(KV, None),
        P(None, "tp"),
        P(None, "tp"),
        P(None, "tp"),
        P(None, "tp"),
        P("tp"),
        P(KV, None),
    )
    return jax.shard_map(
        shards, mesh=split, in_specs=placed, out_specs=P(KV, "tp"), check_vma=False
    )
```

```python
import functools

import jax
import jax.numpy as jnp
from jax import lax
from jax.experimental import pallas as pl
from jax.experimental.pallas import tpu as pltpu
from jax.sharding import Mesh
from jax.sharding import PartitionSpec as P

HEAD = 64
BLOCK = 32
KV = ("z_far", "z_near", "x", "core")
GATHERED = ("z_far", "core")
SELECTED = ("z_near", "x")
FAR_POSITION = 1 << 20
PIECES = 4

VMEM = pl.BlockSpec(memory_space=pltpu.VMEM)
HBM = pl.BlockSpec(memory_space=pltpu.HBM)
SMEM = pl.BlockSpec(memory_space=pltpu.SMEM)
GRANT = pltpu.CompilerParams(vmem_limit_bytes=12 << 20)


def split(number, by):
    return number >> (by.bit_length() - 1), number & (by - 1)


def in_hbm(value):
    return pltpu.with_memory_space_constraint(value, pltpu.HBM)


def prepare_kernel(
    columns,
    cores,
    choice_hbm,
    tokens_hbm,
    key_hbm,
    value_hbm,
    query_hbm,
    slope_hbm,
    listed_hbm,
    rank_ref,
    packed_ref,
    queries_ref,
    choice_ref,
    slope_ref,
    listed_ref,
    place_ref,
    tokens_ref,
    packed_weight_ref,
    query_weight_ref,
    sems,
):
    get_choice, get_slope, put_rank, put_listed = (
        pltpu.make_async_copy(source, target, sems.at[k])
        for k, (source, target) in enumerate(
            (
                (choice_hbm, choice_ref),
                (slope_hbm, slope_ref),
                (place_ref, rank_ref),
                (listed_ref, listed_hbm),
            )
        )
    )
    depth = tokens_ref.shape[1] // PIECES
    pieces = []
    for k in range(PIECES):
        cols = pl.ds(k * depth, depth)
        parts = (
            (tokens_hbm.at[:, cols], tokens_ref.at[:, cols]),
            (key_hbm.at[:, cols], packed_weight_ref.at[pl.ds(0, HEAD), cols]),
            (value_hbm.at[:, cols], packed_weight_ref.at[pl.ds(HEAD, HEAD), cols]),
            (query_hbm.at[cols], query_weight_ref.at[cols]),
        )
        pieces.append(
            [
                pltpu.make_async_copy(source, target, sems.at[4 + 4 * k + n])
                for n, (source, target) in enumerate(parts)
            ]
        )
    get_choice.start()
    for piece in pieces:
        for copy in piece:
            copy.start()
    get_slope.start()
    get_choice.wait()
    blocks_here, topk = choice_ref.shape
    members = lax.axis_size(GATHERED)
    shape = (columns, rank_ref.shape[2])
    column = lax.broadcasted_iota(jnp.int32, shape, 0)
    member = lax.broadcasted_iota(jnp.int32, shape, 1)
    far, core = split(member, cores)
    owner = far * (columns * cores) + column * cores + core
    device, _ = split(choice_ref[0, 0], blocks_here)
    far_owner = (member < members) & (column != split(split(device, cores)[0], columns)[1])
    wanted = jnp.full(shape, -1, jnp.int32)
    for g in range(blocks_here):
        for n in range(1, topk):
            named, local = split(choice_ref[g, n], blocks_here)
            wanted = jnp.where(owner == named, local, wanted)
    wanted = jnp.where(far_owner, wanted, -1)
    needed = wanted >= 0
    upto = needed.astype(jnp.int32)
    step = 1
    while step < members:
        upto = upto + jnp.where(member >= step, pltpu.roll(upto, step, 1), 0)
        step *= 2
    rank = jnp.where(needed, upto - 1, members)
    row = member * blocks_here + wanted
    listed = jnp.full(shape, jnp.max(upto), jnp.int32)
    for place in range(members):
        found = jnp.sum(jnp.where(rank == place, row, 0), axis=1, keepdims=True)
        listed = jnp.where(member == place, found, listed)
    listed_ref[...] = listed.reshape(listed_ref.shape)
    place_ref[...] = rank.reshape(rank_ref.shape)
    put_rank.start()
    put_listed.start()
    packed = queries = 0.0
    for k, piece in enumerate(pieces):
        for copy in piece:
            copy.wait()
        cols = pl.ds(k * depth, depth)
        packed += lax.dot_general(
            tokens_ref[:, cols],
            packed_weight_ref[:, cols],
            (((1,), (1,)), ((), ())),
            preferred_element_type=jnp.float32,
        )
        queries += jnp.dot(
            tokens_ref[:, cols], query_weight_ref[cols], preferred_element_type=jnp.float32
        )
    packed_ref[...] = packed.astype(packed_ref.dtype)
    queries_ref[...] = queries.astype(queries_ref.dtype)
    for copy in (get_slope, put_rank, put_listed):
        copy.wait()


def select_kernel(listed_ref, gathered_ref, outgoing_ref, over_ref):
    columns, places = outgoing_ref.shape[:2]
    longest = listed_ref[0, 0, listed_ref.shape[2] - 1]
    for column in range(1, columns):
        longest = jnp.maximum(longest, listed_ref[column, 0, listed_ref.shape[2] - 1])
    over_ref[0] = (longest > places).astype(jnp.int32)

    @pl.loop(0, columns)
    def _(column):
        for place in range(places):
            outgoing_ref[column, place] = gathered_ref[listed_ref[column, 0, place]]


def attend_kernel(
    cores, choice_ref, slope_ref, rank_ref, queries_ref, gathered_ref, incoming_ref, out_ref
):
    blocks_here, topk = choice_ref.shape
    columns, places = incoming_ref.shape[:2]
    heads = queries_ref.shape[1] // HEAD
    keys = topk * BLOCK
    device, _ = split(choice_ref[0, 0], blocks_here)
    own_column = split(split(device, cores)[0], columns)[1]
    lane = lax.broadcasted_iota(jnp.int32, (BLOCK, 2 * HEAD), 1)
    query_row = lax.broadcasted_iota(jnp.int32, (BLOCK, keys), 0)
    key_lane = lax.broadcasted_iota(jnp.int32, (1, keys), 1)
    for g in range(blocks_here):
        picked = []
        key_pos = jnp.zeros((1, keys), jnp.int32)
        for n in range(topk):
            chosen = choice_ref[g, n]
            safe = jnp.maximum(chosen, 0)
            owner, local = split(safe, blocks_here)
            chip, core = split(owner, cores)
            far, column = split(chip, columns)
            member = far * cores + core
            here = column == own_column
            place = jnp.minimum(rank_ref[column, 0, member], places - 1)
            row = jnp.where(here, member * blocks_here + local, 0)
            block = jnp.where(here, gathered_ref[row], incoming_ref[column, place])
            picked.append(block)
            first = jnp.where(chosen >= 0, chosen * BLOCK, FAR_POSITION)
            key_pos = jnp.where(split(key_lane, BLOCK)[0] == n, first, key_pos)
        table = jnp.concatenate(picked, axis=0)
        key_pos = key_pos + split(key_lane, BLOCK)[1]
        query_pos = (device * blocks_here + g) * BLOCK + query_row
        distance = query_pos - key_pos
        keep = distance >= 0
        far = distance.astype(jnp.float32)
        rows = pl.ds(g * BLOCK, BLOCK)
        padded = []
        for h in range(heads):
            pair = queries_ref[rows, pl.ds(h // 2 * 2 * HEAD, 2 * HEAD)].astype(jnp.float32)
            if h % 2:
                pair = pltpu.roll(pair, HEAD, 1)
            padded.append(jnp.where(lane < HEAD, pair, 0.0).astype(jnp.bfloat16))
        query = jnp.concatenate(padded, axis=0)
        raw = lax.dot_general(
            query, table, (((1,), (1,)), ((), ())), preferred_element_type=jnp.float32
        )
        weights = []
        for h in range(heads):
            scores = raw[h * BLOCK : (h + 1) * BLOCK] * (HEAD**-0.5) - slope_ref[h] * far
            scores = jnp.where(keep, scores, -jnp.inf)
            top = jnp.max(scores, axis=1, keepdims=True)
            expd = jnp.exp(scores - top)
            total = jnp.sum(expd, axis=1, keepdims=True)
            weights.append((expd / total).astype(jnp.bfloat16))
        summed = jnp.dot(
            jnp.concatenate(weights, axis=0), table, preferred_element_type=jnp.float32
        )
        for h in range(0, heads, 2):
            even = pltpu.roll(summed[h * BLOCK : (h + 1) * BLOCK], HEAD, 1)
            odd = summed[(h + 1) * BLOCK : (h + 2) * BLOCK]
            both = jnp.where(lane < HEAD, even, odd).astype(out_ref.dtype)
            for peer in range(out_ref.shape[0]):
                out_ref[peer, rows, pl.ds(h * HEAD, 2 * HEAD)] = both


def mix_kernel(attended_ref, weight_ref, mixed_hbm, mixed_ref, sems):
    peers, _, channels = attended_ref.shape
    width = mixed_ref.shape[2]
    attended = jnp.concatenate([attended_ref[p] for p in range(peers)], axis=1)
    copies = []
    for half in range(2):
        cols = pl.ds(half * width, width)
        mixed = jnp.dot(attended, weight_ref[:, cols], preferred_element_type=jnp.float32)
        mixed_ref[half] = mixed.astype(mixed_ref.dtype)
        copies.append(pltpu.make_async_copy(mixed_ref.at[half], mixed_hbm.at[:, cols], sems.at[half]))
        copies[half].start()
    for copy in copies:
        copy.wait()


def shards(tokens, query_weight, key_weight, value_weight, out_weight, alibi_slope, block_choice):
    rows = tokens.shape[0]
    blocks_here = rows // BLOCK
    columns = lax.axis_size(SELECTED)
    cores = lax.axis_size("core")
    members = lax.axis_size(GATHERED)
    peers = lax.axis_size("tp")
    listed, rank, packed, queries, choice, slope = pl.pallas_call(
        functools.partial(prepare_kernel, columns, cores),
        out_shape=(
            jax.ShapeDtypeStruct((columns, 1, 128), jnp.int32),
            pltpu.SMEM((columns, 1, 128), jnp.int32),
            jax.ShapeDtypeStruct((rows, 2 * HEAD), jnp.bfloat16),
            jax.ShapeDtypeStruct((rows, query_weight.shape[1]), jnp.bfloat16),
            pltpu.SMEM(block_choice.shape, jnp.int32),
            pltpu.SMEM(alibi_slope.shape, jnp.float32),
        ),
        in_specs=[HBM] * 6,
        out_specs=(HBM, SMEM, VMEM, VMEM, SMEM, SMEM),
        scratch_shapes=[
            pltpu.VMEM((columns, 1, 128), jnp.int32),
            pltpu.VMEM((columns, 1, 128), jnp.int32),
            pltpu.VMEM(tokens.shape, jnp.bfloat16),
            pltpu.VMEM((2 * HEAD, tokens.shape[1]), jnp.bfloat16),
            pltpu.VMEM(query_weight.shape, jnp.bfloat16),
            pltpu.SemaphoreType.DMA((4 + 4 * PIECES,)),
        ],
        name="prepare",
        compiler_params=GRANT,
    )(
        in_hbm(block_choice),
        in_hbm(tokens),
        in_hbm(key_weight.T),
        in_hbm(value_weight.T),
        in_hbm(query_weight),
        in_hbm(alibi_slope),
    )
    asked = lax.all_to_all(listed, SELECTED, 0, 0, tiled=True)
    gathered = lax.all_gather(packed, GATHERED, axis=0, tiled=True)
    gathered = gathered.reshape(members * blocks_here, BLOCK, 2 * HEAD)
    def select(places, asked, gathered):
        return pl.pallas_call(
            select_kernel,
            out_shape=(
                jax.ShapeDtypeStruct((columns, places, BLOCK, 2 * HEAD), jnp.bfloat16),
                pltpu.SMEM((1,), jnp.int32),
            ),
            in_specs=[SMEM, VMEM],
            out_specs=(VMEM, SMEM),
            name="select",
            compiler_params=GRANT,
        )(asked, gathered)

    def attend(outgoing, choice, slope, rank, queries, gathered):
        incoming = lax.all_to_all(outgoing, SELECTED, 0, 0, tiled=True)
        return pl.pallas_call(
            functools.partial(attend_kernel, cores),
            out_shape=jax.ShapeDtypeStruct((peers, *queries.shape), jnp.bfloat16),
            in_specs=[SMEM, SMEM, SMEM, VMEM, VMEM, VMEM],
            out_specs=VMEM,
            name="attend",
            compiler_params=GRANT,
        )(choice, slope, rank, queries, gathered, incoming)

    def short_lists(asked, outgoing, *others):
        return attend(outgoing, *others)

    def long_lists(asked, outgoing, *others):
        outgoing, _ = select(members, asked, others[-1])
        return attend(outgoing, *others)

    outgoing, over = select(block_choice.shape[1] - 1, asked, gathered)
    attended = lax.switch(
        over[0],
        (short_lists, long_lists),
        asked,
        outgoing,
        choice,
        slope,
        rank,
        queries,
        gathered,
    )
    everyone = lax.all_to_all(attended, "tp", 0, 0, tiled=True)
    width = out_weight.shape[1]
    return pl.pallas_call(
        mix_kernel,
        out_shape=jax.ShapeDtypeStruct((rows, width), jnp.bfloat16),
        in_specs=[VMEM, VMEM],
        out_specs=HBM,
        scratch_shapes=[
            pltpu.VMEM((2, rows, width // 2), jnp.bfloat16),
            pltpu.SemaphoreType.DMA((2,)),
        ],
        name="mix",
        compiler_params=GRANT,
    )(everyone, out_weight)


def solution(mesh):
    split = Mesh(
        mesh.devices.reshape(8, 2, 4, 2, mesh.shape["tp"]), ("z_far", "z_near", "x", "core", "tp")
    )
    placed = (
        P(KV, None),
        P(None, "tp"),
        P(None, "tp"),
        P(None, "tp"),
        P(None, "tp"),
        P("tp"),
        P(KV, None),
    )
    return jax.shard_map(
        shards, mesh=split, in_specs=placed, out_specs=P(KV, "tp"), check_vma=False
    )
```

```python
import functools

import jax
import jax.numpy as jnp
from jax import lax
from jax.experimental import pallas as pl
from jax.experimental.pallas import tpu as pltpu
from jax.sharding import Mesh
from jax.sharding import PartitionSpec as P

HEAD = 64
BLOCK = 32
KV = ("z_far", "z_near", "x", "core")
GATHERED = ("z_far", "core")
SELECTED = ("z_near", "x")
FAR_POSITION = 1 << 20
PIECES = 4

VMEM = pl.BlockSpec(memory_space=pltpu.VMEM)
HBM = pl.BlockSpec(memory_space=pltpu.HBM)
SMEM = pl.BlockSpec(memory_space=pltpu.SMEM)
GRANT = pltpu.CompilerParams(vmem_limit_bytes=12 << 20)


def split(number, by):
    return number >> (by.bit_length() - 1), number & (by - 1)


def in_hbm(value):
    return pltpu.with_memory_space_constraint(value, pltpu.HBM)


def prepare_kernel(
    columns,
    cores,
    choice_hbm,
    tokens_hbm,
    key_hbm,
    value_hbm,
    query_hbm,
    slope_hbm,
    listed_hbm,
    rank_ref,
    packed_ref,
    queries_ref,
    choice_ref,
    slope_ref,
    listed_ref,
    place_ref,
    tokens_ref,
    packed_weight_ref,
    query_weight_ref,
    sems,
):
    get_choice, get_slope, put_rank, put_listed = (
        pltpu.make_async_copy(source, target, sems.at[k])
        for k, (source, target) in enumerate(
            (
                (choice_hbm, choice_ref),
                (slope_hbm, slope_ref),
                (place_ref, rank_ref),
                (listed_ref, listed_hbm),
            )
        )
    )
    depth = tokens_ref.shape[1] // PIECES
    pieces = []
    for k in range(PIECES):
        cols = pl.ds(k * depth, depth)
        parts = (
            (tokens_hbm.at[:, cols], tokens_ref.at[:, cols]),
            (key_hbm.at[:, cols], packed_weight_ref.at[pl.ds(0, HEAD), cols]),
            (value_hbm.at[:, cols], packed_weight_ref.at[pl.ds(HEAD, HEAD), cols]),
            (query_hbm.at[cols], query_weight_ref.at[cols]),
        )
        pieces.append(
            [
                pltpu.make_async_copy(source, target, sems.at[4 + 4 * k + n])
                for n, (source, target) in enumerate(parts)
            ]
        )
    get_choice.start()
    for piece in pieces:
        for copy in piece:
            copy.start()
    get_slope.start()
    get_choice.wait()
    blocks_here, topk = choice_ref.shape
    members = lax.axis_size(GATHERED)
    shape = (columns, rank_ref.shape[2])
    column = lax.broadcasted_iota(jnp.int32, shape, 0)
    member = lax.broadcasted_iota(jnp.int32, shape, 1)
    far, core = split(member, cores)
    owner = far * (columns * cores) + column * cores + core
    device, _ = split(choice_ref[0, 0], blocks_here)
    far_owner = (member < members) & (column != split(split(device, cores)[0], columns)[1])
    wanted = jnp.full(shape, -1, jnp.int32)
    for g in range(blocks_here):
        for n in range(1, topk):
            named, local = split(choice_ref[g, n], blocks_here)
            wanted = jnp.where(owner == named, local, wanted)
    wanted = jnp.where(far_owner, wanted, -1)
    needed = wanted >= 0
    upto = needed.astype(jnp.int32)
    step = 1
    while step < members:
        upto = upto + jnp.where(member >= step, pltpu.roll(upto, step, 1), 0)
        step *= 2
    rank = jnp.where(needed, upto - 1, members)
    row = member * blocks_here + wanted
    listed = jnp.full(shape, jnp.max(upto), jnp.int32)
    for place in range(members):
        found = jnp.sum(jnp.where(rank == place, row, 0), axis=1, keepdims=True)
        listed = jnp.where(member == place, found, listed)
    listed_ref[...] = listed.reshape(listed_ref.shape)
    place_ref[...] = rank.reshape(rank_ref.shape)
    put_rank.start()
    put_listed.start()
    packed = queries = 0.0
    for k, piece in enumerate(pieces):
        for copy in piece:
            copy.wait()
        cols = pl.ds(k * depth, depth)
        packed += lax.dot_general(
            tokens_ref[:, cols],
            packed_weight_ref[:, cols],
            (((1,), (1,)), ((), ())),
            preferred_element_type=jnp.float32,
        )
        queries += jnp.dot(
            tokens_ref[:, cols], query_weight_ref[cols], preferred_element_type=jnp.float32
        )
    packed_ref[...] = packed.astype(packed_ref.dtype)
    queries_ref[...] = queries.astype(queries_ref.dtype)
    for copy in (get_slope, put_rank, put_listed):
        copy.wait()


def select_kernel(listed_ref, gathered_ref, outgoing_ref, over_ref):
    columns, places = outgoing_ref.shape[:2]
    longest = listed_ref[0, 0, listed_ref.shape[2] - 1]
    for column in range(1, columns):
        longest = jnp.maximum(longest, listed_ref[column, 0, listed_ref.shape[2] - 1])
    over_ref[0] = (longest > places).astype(jnp.int32)

    @pl.loop(0, columns)
    def _(column):
        for place in range(places):
            outgoing_ref[column, place] = gathered_ref[listed_ref[column, 0, place]]


def attend_kernel(
    cores, choice_ref, slope_ref, rank_ref, queries_ref, gathered_ref, incoming_ref, out_ref
):
    blocks_here, topk = choice_ref.shape
    columns, places = incoming_ref.shape[:2]
    heads = queries_ref.shape[1] // HEAD
    keys = topk * BLOCK
    device, _ = split(choice_ref[0, 0], blocks_here)
    own_column = split(split(device, cores)[0], columns)[1]
    lane = lax.broadcasted_iota(jnp.int32, (BLOCK, 2 * HEAD), 1)
    query_row = lax.broadcasted_iota(jnp.int32, (BLOCK, keys), 0)
    key_lane = lax.broadcasted_iota(jnp.int32, (1, keys), 1)
    tables, raws, fars = [], [], []
    for g in range(blocks_here):
        picked = []
        key_pos = jnp.zeros((1, keys), jnp.int32)
        for n in range(topk):
            chosen = choice_ref[g, n]
            safe = jnp.maximum(chosen, 0)
            owner, local = split(safe, blocks_here)
            chip, core = split(owner, cores)
            far, column = split(chip, columns)
            member = far * cores + core
            here = column == own_column
            place = jnp.minimum(rank_ref[column, 0, member], places - 1)
            row = jnp.where(here, member * blocks_here + local, 0)
            block = jnp.where(here, gathered_ref[row], incoming_ref[column, place])
            picked.append(block)
            first = jnp.where(chosen >= 0, chosen * BLOCK, FAR_POSITION)
            key_pos = jnp.where(split(key_lane, BLOCK)[0] == n, first, key_pos)
        table = jnp.concatenate(picked, axis=0)
        key_pos = key_pos + split(key_lane, BLOCK)[1]
        query_pos = (device * blocks_here + g) * BLOCK + query_row
        distance = query_pos - key_pos
        fars.append(jnp.where(distance >= 0, distance.astype(jnp.float32), jnp.inf))
        rows = pl.ds(g * BLOCK, BLOCK)
        padded = []
        for h in range(heads):
            pair = queries_ref[rows, pl.ds(h // 2 * 2 * HEAD, 2 * HEAD)].astype(jnp.float32)
            if h % 2:
                pair = pltpu.roll(pair, HEAD, 1)
            padded.append(jnp.where(lane < HEAD, pair, 0.0).astype(jnp.bfloat16))
        query = jnp.concatenate(padded, axis=0)
        raws.append(
            lax.dot_general(
                query, table, (((1,), (1,)), ((), ())), preferred_element_type=jnp.float32
            )
        )
        tables.append(table)
    sums = []
    for table, raw, far in zip(tables, raws, fars):
        weights = []
        for h in range(heads):
            scores = raw[h * BLOCK : (h + 1) * BLOCK] * (HEAD**-0.5) - slope_ref[h] * far
            top = jnp.max(scores, axis=1, keepdims=True)
            expd = jnp.exp(scores - top)
            total = jnp.sum(expd, axis=1, keepdims=True)
            weights.append((expd / total).astype(jnp.bfloat16))
        sums.append(
            jnp.dot(jnp.concatenate(weights, axis=0), table, preferred_element_type=jnp.float32)
        )
    for g, summed in enumerate(sums):
        rows = pl.ds(g * BLOCK, BLOCK)
        for h in range(0, heads, 2):
            even = pltpu.roll(summed[h * BLOCK : (h + 1) * BLOCK], HEAD, 1)
            odd = summed[(h + 1) * BLOCK : (h + 2) * BLOCK]
            both = jnp.where(lane < HEAD, even, odd).astype(out_ref.dtype)
            for peer in range(out_ref.shape[0]):
                out_ref[peer, rows, pl.ds(h * HEAD, 2 * HEAD)] = both


def mix_kernel(attended_ref, weight_ref, mixed_hbm, mixed_ref, sems):
    peers, _, channels = attended_ref.shape
    width = mixed_ref.shape[2]
    attended = jnp.concatenate([attended_ref[p] for p in range(peers)], axis=1)
    copies = []
    for half in range(2):
        cols = pl.ds(half * width, width)
        mixed = jnp.dot(attended, weight_ref[:, cols], preferred_element_type=jnp.float32)
        mixed_ref[half] = mixed.astype(mixed_ref.dtype)
        copies.append(pltpu.make_async_copy(mixed_ref.at[half], mixed_hbm.at[:, cols], sems.at[half]))
        copies[half].start()
    for copy in copies:
        copy.wait()


def shards(tokens, query_weight, key_weight, value_weight, out_weight, alibi_slope, block_choice):
    rows = tokens.shape[0]
    blocks_here = rows // BLOCK
    columns = lax.axis_size(SELECTED)
    cores = lax.axis_size("core")
    members = lax.axis_size(GATHERED)
    peers = lax.axis_size("tp")
    listed, rank, packed, queries, choice, slope = pl.pallas_call(
        functools.partial(prepare_kernel, columns, cores),
        out_shape=(
            jax.ShapeDtypeStruct((columns, 1, 128), jnp.int32),
            pltpu.SMEM((columns, 1, 128), jnp.int32),
            jax.ShapeDtypeStruct((rows, 2 * HEAD), jnp.bfloat16),
            jax.ShapeDtypeStruct((rows, query_weight.shape[1]), jnp.bfloat16),
            pltpu.SMEM(block_choice.shape, jnp.int32),
            pltpu.SMEM(alibi_slope.shape, jnp.float32),
        ),
        in_specs=[HBM] * 6,
        out_specs=(HBM, SMEM, VMEM, VMEM, SMEM, SMEM),
        scratch_shapes=[
            pltpu.VMEM((columns, 1, 128), jnp.int32),
            pltpu.VMEM((columns, 1, 128), jnp.int32),
            pltpu.VMEM(tokens.shape, jnp.bfloat16),
            pltpu.VMEM((2 * HEAD, tokens.shape[1]), jnp.bfloat16),
            pltpu.VMEM(query_weight.shape, jnp.bfloat16),
            pltpu.SemaphoreType.DMA((4 + 4 * PIECES,)),
        ],
        name="prepare",
        compiler_params=GRANT,
    )(
        in_hbm(block_choice),
        in_hbm(tokens),
        in_hbm(key_weight.T),
        in_hbm(value_weight.T),
        in_hbm(query_weight),
        in_hbm(alibi_slope),
    )
    asked = lax.all_to_all(listed, SELECTED, 0, 0, tiled=True)
    gathered = lax.all_gather(packed, GATHERED, axis=0, tiled=True)
    gathered = gathered.reshape(members * blocks_here, BLOCK, 2 * HEAD)
    def select(places, asked, gathered):
        return pl.pallas_call(
            select_kernel,
            out_shape=(
                jax.ShapeDtypeStruct((columns, places, BLOCK, 2 * HEAD), jnp.bfloat16),
                pltpu.SMEM((1,), jnp.int32),
            ),
            in_specs=[SMEM, VMEM],
            out_specs=(VMEM, SMEM),
            name="select",
            compiler_params=GRANT,
        )(asked, gathered)

    def attend(outgoing, choice, slope, rank, queries, gathered):
        incoming = lax.all_to_all(outgoing, SELECTED, 0, 0, tiled=True)
        return pl.pallas_call(
            functools.partial(attend_kernel, cores),
            out_shape=jax.ShapeDtypeStruct((peers, *queries.shape), jnp.bfloat16),
            in_specs=[SMEM, SMEM, SMEM, VMEM, VMEM, VMEM],
            out_specs=VMEM,
            name="attend",
            compiler_params=GRANT,
        )(choice, slope, rank, queries, gathered, incoming)

    def short_lists(asked, outgoing, *others):
        return attend(outgoing, *others)

    def long_lists(asked, outgoing, *others):
        outgoing, _ = select(members, asked, others[-1])
        return attend(outgoing, *others)

    outgoing, over = select(block_choice.shape[1] - 1, asked, gathered)
    attended = lax.switch(
        over[0],
        (short_lists, long_lists),
        asked,
        outgoing,
        choice,
        slope,
        rank,
        queries,
        gathered,
    )
    everyone = lax.all_to_all(attended, "tp", 0, 0, tiled=True)
    width = out_weight.shape[1]
    return pl.pallas_call(
        mix_kernel,
        out_shape=jax.ShapeDtypeStruct((rows, width), jnp.bfloat16),
        in_specs=[VMEM, VMEM],
        out_specs=HBM,
        scratch_shapes=[
            pltpu.VMEM((2, rows, width // 2), jnp.bfloat16),
            pltpu.SemaphoreType.DMA((2,)),
        ],
        name="mix",
        compiler_params=GRANT,
    )(everyone, out_weight)


def solution(mesh):
    split = Mesh(
        mesh.devices.reshape(8, 2, 4, 2, mesh.shape["tp"]), ("z_far", "z_near", "x", "core", "tp")
    )
    placed = (
        P(KV, None),
        P(None, "tp"),
        P(None, "tp"),
        P(None, "tp"),
        P(None, "tp"),
        P("tp"),
        P(KV, None),
    )
    return jax.shard_map(
        shards, mesh=split, in_specs=placed, out_specs=P(KV, "tp"), check_vma=False
    )
```

```python
import functools

import jax
import jax.numpy as jnp
from jax import lax
from jax.experimental import pallas as pl
from jax.experimental.pallas import tpu as pltpu
from jax.sharding import Mesh
from jax.sharding import PartitionSpec as P

HEAD = 64
BLOCK = 32
KV = ("z_far", "z_near", "x", "core")
GATHERED = ("z_far", "core")
SELECTED = ("z_near", "x")
FAR_POSITION = 1 << 20
PIECES = 4

VMEM = pl.BlockSpec(memory_space=pltpu.VMEM)
HBM = pl.BlockSpec(memory_space=pltpu.HBM)
SMEM = pl.BlockSpec(memory_space=pltpu.SMEM)
GRANT = pltpu.CompilerParams(vmem_limit_bytes=12 << 20)


def split(number, by):
    return number >> (by.bit_length() - 1), number & (by - 1)


def in_hbm(value):
    return pltpu.with_memory_space_constraint(value, pltpu.HBM)


def prepare_kernel(
    columns,
    cores,
    choice_hbm,
    tokens_hbm,
    key_hbm,
    value_hbm,
    query_hbm,
    slope_hbm,
    listed_hbm,
    rank_ref,
    packed_ref,
    queries_ref,
    choice_ref,
    slope_ref,
    listed_ref,
    place_ref,
    tokens_ref,
    packed_weight_ref,
    query_weight_ref,
    sems,
):
    get_choice, get_slope, put_rank, put_listed = (
        pltpu.make_async_copy(source, target, sems.at[k])
        for k, (source, target) in enumerate(
            (
                (choice_hbm, choice_ref),
                (slope_hbm, slope_ref),
                (place_ref, rank_ref),
                (listed_ref, listed_hbm),
            )
        )
    )
    depth = tokens_ref.shape[1] // PIECES
    pieces = []
    for k in range(PIECES):
        cols = pl.ds(k * depth, depth)
        parts = (
            (tokens_hbm.at[:, cols], tokens_ref.at[:, cols]),
            (key_hbm.at[:, cols], packed_weight_ref.at[pl.ds(0, HEAD), cols]),
            (value_hbm.at[:, cols], packed_weight_ref.at[pl.ds(HEAD, HEAD), cols]),
            (query_hbm.at[cols], query_weight_ref.at[cols]),
        )
        pieces.append(
            [
                pltpu.make_async_copy(source, target, sems.at[4 + 4 * k + n])
                for n, (source, target) in enumerate(parts)
            ]
        )
    get_choice.start()
    for piece in pieces:
        for copy in piece:
            copy.start()
    get_slope.start()
    get_choice.wait()
    blocks_here, topk = choice_ref.shape
    members = lax.axis_size(GATHERED)
    shape = (columns, rank_ref.shape[2])
    column = lax.broadcasted_iota(jnp.int32, shape, 0)
    member = lax.broadcasted_iota(jnp.int32, shape, 1)
    far, core = split(member, cores)
    owner = far * (columns * cores) + column * cores + core
    device, _ = split(choice_ref[0, 0], blocks_here)
    far_owner = (member < members) & (column != split(split(device, cores)[0], columns)[1])
    wanted = jnp.full(shape, -1, jnp.int32)
    for g in range(blocks_here):
        for n in range(1, topk):
            named, local = split(choice_ref[g, n], blocks_here)
            wanted = jnp.where(owner == named, local, wanted)
    wanted = jnp.where(far_owner, wanted, -1)
    needed = wanted >= 0
    upto = needed.astype(jnp.int32)
    step = 1
    while step < members:
        upto = upto + jnp.where(member >= step, pltpu.roll(upto, step, 1), 0)
        step *= 2
    rank = jnp.where(needed, upto - 1, members)
    row = member * blocks_here + wanted
    listed = jnp.full(shape, jnp.max(upto), jnp.int32)
    for place in range(members):
        found = jnp.sum(jnp.where(rank == place, row, 0), axis=1, keepdims=True)
        listed = jnp.where(member == place, found, listed)
    listed_ref[...] = listed.reshape(listed_ref.shape)
    place_ref[...] = rank.reshape(rank_ref.shape)
    put_rank.start()
    put_listed.start()
    packed = queries = 0.0
    for k, piece in enumerate(pieces):
        for copy in piece:
            copy.wait()
        cols = pl.ds(k * depth, depth)
        packed += lax.dot_general(
            tokens_ref[:, cols],
            packed_weight_ref[:, cols],
            (((1,), (1,)), ((), ())),
            preferred_element_type=jnp.float32,
        )
        queries += jnp.dot(
            tokens_ref[:, cols], query_weight_ref[cols], preferred_element_type=jnp.float32
        )
    packed_ref[...] = packed.astype(packed_ref.dtype)
    queries_ref[...] = queries.astype(queries_ref.dtype)
    for copy in (get_slope, put_rank, put_listed):
        copy.wait()


def select_kernel(listed_ref, gathered_ref, outgoing_ref, over_ref):
    columns, places = outgoing_ref.shape[:2]
    longest = listed_ref[0, 0, listed_ref.shape[2] - 1]
    for column in range(1, columns):
        longest = jnp.maximum(longest, listed_ref[column, 0, listed_ref.shape[2] - 1])
    over_ref[0] = (longest > places).astype(jnp.int32)

    for column in range(columns):
        blocks = [gathered_ref[listed_ref[column, 0, place]] for place in range(places)]
        for place, block in enumerate(blocks):
            outgoing_ref[column, place] = block


def attend_kernel(
    cores, choice_ref, slope_ref, rank_ref, queries_ref, gathered_ref, incoming_ref, out_ref
):
    blocks_here, topk = choice_ref.shape
    columns, places = incoming_ref.shape[:2]
    heads = queries_ref.shape[1] // HEAD
    keys = topk * BLOCK
    device, _ = split(choice_ref[0, 0], blocks_here)
    own_column = split(split(device, cores)[0], columns)[1]
    lane = lax.broadcasted_iota(jnp.int32, (BLOCK, 2 * HEAD), 1)
    query_row = lax.broadcasted_iota(jnp.int32, (BLOCK, keys), 0)
    key_lane = lax.broadcasted_iota(jnp.int32, (1, keys), 1)
    tables, raws, fars = [], [], []
    for g in range(blocks_here):
        picked = []
        key_pos = jnp.zeros((1, keys), jnp.int32)
        for n in range(topk):
            chosen = choice_ref[g, n]
            safe = jnp.maximum(chosen, 0)
            owner, local = split(safe, blocks_here)
            chip, core = split(owner, cores)
            far, column = split(chip, columns)
            member = far * cores + core
            here = column == own_column
            place = jnp.minimum(rank_ref[column, 0, member], places - 1)
            row = jnp.where(here, member * blocks_here + local, 0)
            block = jnp.where(here, gathered_ref[row], incoming_ref[column, place])
            picked.append(block)
            first = jnp.where(chosen >= 0, chosen * BLOCK, FAR_POSITION)
            key_pos = jnp.where(split(key_lane, BLOCK)[0] == n, first, key_pos)
        table = jnp.concatenate(picked, axis=0)
        key_pos = key_pos + split(key_lane, BLOCK)[1]
        query_pos = (device * blocks_here + g) * BLOCK + query_row
        distance = query_pos - key_pos
        fars.append(jnp.where(distance >= 0, distance.astype(jnp.float32), jnp.inf))
        rows = pl.ds(g * BLOCK, BLOCK)
        padded = []
        for h in range(heads):
            pair = queries_ref[rows, pl.ds(h // 2 * 2 * HEAD, 2 * HEAD)].astype(jnp.float32)
            if h % 2:
                pair = pltpu.roll(pair, HEAD, 1)
            padded.append(jnp.where(lane < HEAD, pair, 0.0).astype(jnp.bfloat16))
        query = jnp.concatenate(padded, axis=0)
        raws.append(
            lax.dot_general(
                query, table, (((1,), (1,)), ((), ())), preferred_element_type=jnp.float32
            )
        )
        tables.append(table)
    sums = []
    for table, raw, far in zip(tables, raws, fars):
        weights = []
        for h in range(heads):
            scores = raw[h * BLOCK : (h + 1) * BLOCK] * (HEAD**-0.5) - slope_ref[h] * far
            top = jnp.max(scores, axis=1, keepdims=True)
            expd = jnp.exp(scores - top)
            total = jnp.sum(expd, axis=1, keepdims=True)
            weights.append((expd / total).astype(jnp.bfloat16))
        sums.append(
            jnp.dot(jnp.concatenate(weights, axis=0), table, preferred_element_type=jnp.float32)
        )
    for g, summed in enumerate(sums):
        rows = pl.ds(g * BLOCK, BLOCK)
        for h in range(0, heads, 2):
            even = pltpu.roll(summed[h * BLOCK : (h + 1) * BLOCK], HEAD, 1)
            odd = summed[(h + 1) * BLOCK : (h + 2) * BLOCK]
            both = jnp.where(lane < HEAD, even, odd).astype(out_ref.dtype)
            for peer in range(out_ref.shape[0]):
                out_ref[peer, rows, pl.ds(h * HEAD, 2 * HEAD)] = both


def mix_kernel(attended_ref, weight_ref, mixed_hbm, mixed_ref, sems):
    peers, _, channels = attended_ref.shape
    width = mixed_ref.shape[2]
    attended = jnp.concatenate([attended_ref[p] for p in range(peers)], axis=1)
    copies = []
    for half in range(2):
        cols = pl.ds(half * width, width)
        mixed = jnp.dot(attended, weight_ref[:, cols], preferred_element_type=jnp.float32)
        mixed_ref[half] = mixed.astype(mixed_ref.dtype)
        copies.append(pltpu.make_async_copy(mixed_ref.at[half], mixed_hbm.at[:, cols], sems.at[half]))
        copies[half].start()
    for copy in copies:
        copy.wait()


def shards(tokens, query_weight, key_weight, value_weight, out_weight, alibi_slope, block_choice):
    rows = tokens.shape[0]
    blocks_here = rows // BLOCK
    columns = lax.axis_size(SELECTED)
    cores = lax.axis_size("core")
    members = lax.axis_size(GATHERED)
    peers = lax.axis_size("tp")
    listed, rank, packed, queries, choice, slope = pl.pallas_call(
        functools.partial(prepare_kernel, columns, cores),
        out_shape=(
            jax.ShapeDtypeStruct((columns, 1, 128), jnp.int32),
            pltpu.SMEM((columns, 1, 128), jnp.int32),
            jax.ShapeDtypeStruct((rows, 2 * HEAD), jnp.bfloat16),
            jax.ShapeDtypeStruct((rows, query_weight.shape[1]), jnp.bfloat16),
            pltpu.SMEM(block_choice.shape, jnp.int32),
            pltpu.SMEM(alibi_slope.shape, jnp.float32),
        ),
        in_specs=[HBM] * 6,
        out_specs=(HBM, SMEM, VMEM, VMEM, SMEM, SMEM),
        scratch_shapes=[
            pltpu.VMEM((columns, 1, 128), jnp.int32),
            pltpu.VMEM((columns, 1, 128), jnp.int32),
            pltpu.VMEM(tokens.shape, jnp.bfloat16),
            pltpu.VMEM((2 * HEAD, tokens.shape[1]), jnp.bfloat16),
            pltpu.VMEM(query_weight.shape, jnp.bfloat16),
            pltpu.SemaphoreType.DMA((4 + 4 * PIECES,)),
        ],
        name="prepare",
        compiler_params=GRANT,
    )(
        in_hbm(block_choice),
        in_hbm(tokens),
        in_hbm(key_weight.T),
        in_hbm(value_weight.T),
        in_hbm(query_weight),
        in_hbm(alibi_slope),
    )
    asked = lax.all_to_all(listed, SELECTED, 0, 0, tiled=True)
    gathered = lax.all_gather(packed, GATHERED, axis=0, tiled=True)
    gathered = gathered.reshape(members * blocks_here, BLOCK, 2 * HEAD)
    def select(places, asked, gathered):
        return pl.pallas_call(
            select_kernel,
            out_shape=(
                jax.ShapeDtypeStruct((columns, places, BLOCK, 2 * HEAD), jnp.bfloat16),
                pltpu.SMEM((1,), jnp.int32),
            ),
            in_specs=[SMEM, VMEM],
            out_specs=(VMEM, SMEM),
            name="select",
            compiler_params=GRANT,
        )(asked, gathered)

    def attend(outgoing, choice, slope, rank, queries, gathered):
        incoming = lax.all_to_all(outgoing, SELECTED, 0, 0, tiled=True)
        return pl.pallas_call(
            functools.partial(attend_kernel, cores),
            out_shape=jax.ShapeDtypeStruct((peers, *queries.shape), jnp.bfloat16),
            in_specs=[SMEM, SMEM, SMEM, VMEM, VMEM, VMEM],
            out_specs=VMEM,
            name="attend",
            compiler_params=GRANT,
        )(choice, slope, rank, queries, gathered, incoming)

    def short_lists(asked, outgoing, *others):
        return attend(outgoing, *others)

    def long_lists(asked, outgoing, *others):
        outgoing, _ = select(members, asked, others[-1])
        return attend(outgoing, *others)

    outgoing, over = select(block_choice.shape[1] - 1, asked, gathered)
    attended = lax.switch(
        over[0],
        (short_lists, long_lists),
        asked,
        outgoing,
        choice,
        slope,
        rank,
        queries,
        gathered,
    )
    everyone = lax.all_to_all(attended, "tp", 0, 0, tiled=True)
    width = out_weight.shape[1]
    return pl.pallas_call(
        mix_kernel,
        out_shape=jax.ShapeDtypeStruct((rows, width), jnp.bfloat16),
        in_specs=[VMEM, VMEM],
        out_specs=HBM,
        scratch_shapes=[
            pltpu.VMEM((2, rows, width // 2), jnp.bfloat16),
            pltpu.SemaphoreType.DMA((2,)),
        ],
        name="mix",
        compiler_params=GRANT,
    )(everyone, out_weight)


def solution(mesh):
    split = Mesh(
        mesh.devices.reshape(8, 2, 4, 2, mesh.shape["tp"]), ("z_far", "z_near", "x", "core", "tp")
    )
    placed = (
        P(KV, None),
        P(None, "tp"),
        P(None, "tp"),
        P(None, "tp"),
        P(None, "tp"),
        P("tp"),
        P(KV, None),
    )
    return jax.shard_map(
        shards, mesh=split, in_specs=placed, out_specs=P(KV, "tp"), check_vma=False
    )
```

```python
import functools

import jax
import jax.numpy as jnp
from jax import lax
from jax.experimental import pallas as pl
from jax.experimental.pallas import tpu as pltpu
from jax.sharding import Mesh
from jax.sharding import PartitionSpec as P

HEAD = 64
BLOCK = 32
KV = ("z_far", "z_near", "x", "core")
GATHERED = ("z_far", "core")
SELECTED = ("z_near", "x")
FAR_POSITION = 1 << 20
PIECES = 4

VMEM = pl.BlockSpec(memory_space=pltpu.VMEM)
HBM = pl.BlockSpec(memory_space=pltpu.HBM)
SMEM = pl.BlockSpec(memory_space=pltpu.SMEM)
GRANT = pltpu.CompilerParams(vmem_limit_bytes=12 << 20)


def split(number, by):
    return number >> (by.bit_length() - 1), number & (by - 1)


def in_hbm(value):
    return pltpu.with_memory_space_constraint(value, pltpu.HBM)


def prepare_kernel(
    columns,
    cores,
    choice_hbm,
    tokens_hbm,
    key_hbm,
    value_hbm,
    query_hbm,
    slope_hbm,
    listed_hbm,
    rank_ref,
    packed_ref,
    queries_ref,
    choice_ref,
    slope_ref,
    listed_ref,
    place_ref,
    tokens_ref,
    packed_weight_ref,
    query_weight_ref,
    sems,
):
    get_choice, get_slope, put_rank, put_listed = (
        pltpu.make_async_copy(source, target, sems.at[k])
        for k, (source, target) in enumerate(
            (
                (choice_hbm, choice_ref),
                (slope_hbm, slope_ref),
                (place_ref, rank_ref),
                (listed_ref, listed_hbm),
            )
        )
    )
    depth = tokens_ref.shape[1] // PIECES
    pieces = []
    for k in range(PIECES):
        cols = pl.ds(k * depth, depth)
        parts = ()
        if k == 0:
            parts = (
                (key_hbm, packed_weight_ref.at[pl.ds(0, HEAD)]),
                (value_hbm, packed_weight_ref.at[pl.ds(HEAD, HEAD)]),
            )
        parts += (
            (tokens_hbm.at[:, cols], tokens_ref.at[:, cols]),
            (query_hbm.at[cols], query_weight_ref.at[cols]),
        )
        pieces.append(
            [
                pltpu.make_async_copy(source, target, sems.at[4 + 4 * k + n])
                for n, (source, target) in enumerate(parts)
            ]
        )
    get_choice.start()
    for piece in pieces:
        for copy in piece:
            copy.start()
    get_slope.start()
    get_choice.wait()
    blocks_here, topk = choice_ref.shape
    members = lax.axis_size(GATHERED)
    shape = (columns, rank_ref.shape[2])
    column = lax.broadcasted_iota(jnp.int32, shape, 0)
    member = lax.broadcasted_iota(jnp.int32, shape, 1)
    far, core = split(member, cores)
    owner = far * (columns * cores) + column * cores + core
    device, _ = split(choice_ref[0, 0], blocks_here)
    far_owner = (member < members) & (column != split(split(device, cores)[0], columns)[1])
    wanted = jnp.full(shape, -1, jnp.int32)
    for g in range(blocks_here):
        for n in range(1, topk):
            named, local = split(choice_ref[g, n], blocks_here)
            wanted = jnp.where(owner == named, local, wanted)
    wanted = jnp.where(far_owner, wanted, -1)
    needed = wanted >= 0
    upto = needed.astype(jnp.int32)
    step = 1
    while step < members:
        upto = upto + jnp.where(member >= step, pltpu.roll(upto, step, 1), 0)
        step *= 2
    rank = jnp.where(needed, upto - 1, members)
    row = member * blocks_here + wanted
    listed = jnp.full(shape, jnp.max(upto), jnp.int32)
    for place in range(members):
        found = jnp.sum(jnp.where(rank == place, row, 0), axis=1, keepdims=True)
        listed = jnp.where(member == place, found, listed)
    listed_ref[...] = listed.reshape(listed_ref.shape)
    place_ref[...] = rank.reshape(rank_ref.shape)
    put_rank.start()
    put_listed.start()
    packed = queries = 0.0
    for k, piece in enumerate(pieces):
        for copy in piece:
            copy.wait()
        cols = pl.ds(k * depth, depth)
        packed += lax.dot_general(
            tokens_ref[:, cols],
            packed_weight_ref[:, cols],
            (((1,), (1,)), ((), ())),
            preferred_element_type=jnp.float32,
        )
        queries += jnp.dot(
            tokens_ref[:, cols], query_weight_ref[cols], preferred_element_type=jnp.float32
        )
    packed_ref[...] = packed.astype(packed_ref.dtype)
    queries_ref[...] = queries.astype(queries_ref.dtype)
    for copy in (get_slope, put_rank, put_listed):
        copy.wait()


def select_kernel(listed_ref, gathered_ref, outgoing_ref, over_ref):
    columns, places = outgoing_ref.shape[:2]
    longest = listed_ref[0, 0, listed_ref.shape[2] - 1]
    for column in range(1, columns):
        longest = jnp.maximum(longest, listed_ref[column, 0, listed_ref.shape[2] - 1])
    over_ref[0] = (longest > places).astype(jnp.int32)

    for column in range(columns):
        blocks = [gathered_ref[listed_ref[column, 0, place]] for place in range(places)]
        for place, block in enumerate(blocks):
            outgoing_ref[column, place] = block


def attend_kernel(
    cores, choice_ref, slope_ref, rank_ref, queries_ref, gathered_ref, incoming_ref, out_ref
):
    blocks_here, topk = choice_ref.shape
    columns, places = incoming_ref.shape[:2]
    heads = queries_ref.shape[1] // HEAD
    keys = topk * BLOCK
    device, _ = split(choice_ref[0, 0], blocks_here)
    own_column = split(split(device, cores)[0], columns)[1]
    lane = lax.broadcasted_iota(jnp.int32, (BLOCK, 2 * HEAD), 1)
    query_row = lax.broadcasted_iota(jnp.int32, (BLOCK, keys), 0)
    key_lane = lax.broadcasted_iota(jnp.int32, (1, keys), 1)
    tables, raws, fars = [], [], []
    for g in range(blocks_here):
        picked = []
        key_pos = jnp.zeros((1, keys), jnp.int32)
        for n in range(topk):
            chosen = choice_ref[g, n]
            safe = jnp.maximum(chosen, 0)
            owner, local = split(safe, blocks_here)
            chip, core = split(owner, cores)
            far, column = split(chip, columns)
            member = far * cores + core
            here = column == own_column
            place = jnp.minimum(rank_ref[column, 0, member], places - 1)
            row = jnp.where(here, member * blocks_here + local, 0)
            block = jnp.where(here, gathered_ref[row], incoming_ref[column, place])
            picked.append(block)
            first = jnp.where(chosen >= 0, chosen * BLOCK, FAR_POSITION)
            key_pos = jnp.where(split(key_lane, BLOCK)[0] == n, first, key_pos)
        table = jnp.concatenate(picked, axis=0)
        key_pos = key_pos + split(key_lane, BLOCK)[1]
        query_pos = (device * blocks_here + g) * BLOCK + query_row
        distance = query_pos - key_pos
        fars.append(jnp.where(distance >= 0, distance.astype(jnp.float32), jnp.inf))
        rows = pl.ds(g * BLOCK, BLOCK)
        padded = []
        for h in range(heads):
            pair = queries_ref[rows, pl.ds(h // 2 * 2 * HEAD, 2 * HEAD)].astype(jnp.float32)
            if h % 2:
                pair = pltpu.roll(pair, HEAD, 1)
            padded.append(jnp.where(lane < HEAD, pair, 0.0).astype(jnp.bfloat16))
        query = jnp.concatenate(padded, axis=0)
        raws.append(
            lax.dot_general(
                query, table, (((1,), (1,)), ((), ())), preferred_element_type=jnp.float32
            )
        )
        tables.append(table)
    sums = []
    for table, raw, far in zip(tables, raws, fars):
        weights = []
        for h in range(heads):
            scores = raw[h * BLOCK : (h + 1) * BLOCK] * (HEAD**-0.5) - slope_ref[h] * far
            top = jnp.max(scores, axis=1, keepdims=True)
            expd = jnp.exp(scores - top)
            total = jnp.sum(expd, axis=1, keepdims=True)
            weights.append((expd / total).astype(jnp.bfloat16))
        sums.append(
            jnp.dot(jnp.concatenate(weights, axis=0), table, preferred_element_type=jnp.float32)
        )
    for g, summed in enumerate(sums):
        rows = pl.ds(g * BLOCK, BLOCK)
        for h in range(0, heads, 2):
            even = pltpu.roll(summed[h * BLOCK : (h + 1) * BLOCK], HEAD, 1)
            odd = summed[(h + 1) * BLOCK : (h + 2) * BLOCK]
            both = jnp.where(lane < HEAD, even, odd).astype(out_ref.dtype)
            for peer in range(out_ref.shape[0]):
                out_ref[peer, rows, pl.ds(h * HEAD, 2 * HEAD)] = both


def mix_kernel(attended_ref, weight_ref, mixed_hbm, mixed_ref, sems):
    peers, _, channels = attended_ref.shape
    width = mixed_ref.shape[2]
    attended = jnp.concatenate([attended_ref[p] for p in range(peers)], axis=1)
    copies = []
    for half in range(2):
        cols = pl.ds(half * width, width)
        mixed = jnp.dot(attended, weight_ref[:, cols], preferred_element_type=jnp.float32)
        mixed_ref[half] = mixed.astype(mixed_ref.dtype)
        copies.append(pltpu.make_async_copy(mixed_ref.at[half], mixed_hbm.at[:, cols], sems.at[half]))
        copies[half].start()
    for copy in copies:
        copy.wait()


def shards(tokens, query_weight, key_weight, value_weight, out_weight, alibi_slope, block_choice):
    rows = tokens.shape[0]
    blocks_here = rows // BLOCK
    columns = lax.axis_size(SELECTED)
    cores = lax.axis_size("core")
    members = lax.axis_size(GATHERED)
    peers = lax.axis_size("tp")
    listed, rank, packed, queries, choice, slope = pl.pallas_call(
        functools.partial(prepare_kernel, columns, cores),
        out_shape=(
            jax.ShapeDtypeStruct((columns, 1, 128), jnp.int32),
            pltpu.SMEM((columns, 1, 128), jnp.int32),
            jax.ShapeDtypeStruct((rows, 2 * HEAD), jnp.bfloat16),
            jax.ShapeDtypeStruct((rows, query_weight.shape[1]), jnp.bfloat16),
            pltpu.SMEM(block_choice.shape, jnp.int32),
            pltpu.SMEM(alibi_slope.shape, jnp.float32),
        ),
        in_specs=[HBM] * 6,
        out_specs=(HBM, SMEM, VMEM, VMEM, SMEM, SMEM),
        scratch_shapes=[
            pltpu.VMEM((columns, 1, 128), jnp.int32),
            pltpu.VMEM((columns, 1, 128), jnp.int32),
            pltpu.VMEM(tokens.shape, jnp.bfloat16),
            pltpu.VMEM((2 * HEAD, tokens.shape[1]), jnp.bfloat16),
            pltpu.VMEM(query_weight.shape, jnp.bfloat16),
            pltpu.SemaphoreType.DMA((4 + 4 * PIECES,)),
        ],
        name="prepare",
        compiler_params=GRANT,
    )(
        in_hbm(block_choice),
        in_hbm(tokens),
        in_hbm(key_weight.T),
        in_hbm(value_weight.T),
        in_hbm(query_weight),
        in_hbm(alibi_slope),
    )
    asked = lax.all_to_all(listed, SELECTED, 0, 0, tiled=True)
    gathered = lax.all_gather(packed, GATHERED, axis=0, tiled=True)
    gathered = gathered.reshape(members * blocks_here, BLOCK, 2 * HEAD)
    def select(places, asked, gathered):
        return pl.pallas_call(
            select_kernel,
            out_shape=(
                jax.ShapeDtypeStruct((columns, places, BLOCK, 2 * HEAD), jnp.bfloat16),
                pltpu.SMEM((1,), jnp.int32),
            ),
            in_specs=[SMEM, VMEM],
            out_specs=(VMEM, SMEM),
            name="select",
            compiler_params=GRANT,
        )(asked, gathered)

    def attend(outgoing, choice, slope, rank, queries, gathered):
        incoming = lax.all_to_all(outgoing, SELECTED, 0, 0, tiled=True)
        return pl.pallas_call(
            functools.partial(attend_kernel, cores),
            out_shape=jax.ShapeDtypeStruct((peers, *queries.shape), jnp.bfloat16),
            in_specs=[SMEM, SMEM, SMEM, VMEM, VMEM, VMEM],
            out_specs=VMEM,
            name="attend",
            compiler_params=GRANT,
        )(choice, slope, rank, queries, gathered, incoming)

    def short_lists(asked, outgoing, *others):
        return attend(outgoing, *others)

    def long_lists(asked, outgoing, *others):
        outgoing, _ = select(members, asked, others[-1])
        return attend(outgoing, *others)

    outgoing, over = select(block_choice.shape[1] - 1, asked, gathered)
    attended = lax.switch(
        over[0],
        (short_lists, long_lists),
        asked,
        outgoing,
        choice,
        slope,
        rank,
        queries,
        gathered,
    )
    everyone = lax.all_to_all(attended, "tp", 0, 0, tiled=True)
    width = out_weight.shape[1]
    return pl.pallas_call(
        mix_kernel,
        out_shape=jax.ShapeDtypeStruct((rows, width), jnp.bfloat16),
        in_specs=[VMEM, VMEM],
        out_specs=HBM,
        scratch_shapes=[
            pltpu.VMEM((2, rows, width // 2), jnp.bfloat16),
            pltpu.SemaphoreType.DMA((2,)),
        ],
        name="mix",
        compiler_params=GRANT,
    )(everyone, out_weight)


def solution(mesh):
    split = Mesh(
        mesh.devices.reshape(8, 2, 4, 2, mesh.shape["tp"]), ("z_far", "z_near", "x", "core", "tp")
    )
    placed = (
        P(KV, None),
        P(None, "tp"),
        P(None, "tp"),
        P(None, "tp"),
        P(None, "tp"),
        P("tp"),
        P(KV, None),
    )
    return jax.shard_map(
        shards, mesh=split, in_specs=placed, out_specs=P(KV, "tp"), check_vma=False
    )
```

```python
import functools

import jax
import jax.numpy as jnp
from jax import lax
from jax.experimental import pallas as pl
from jax.experimental.pallas import tpu as pltpu
from jax.sharding import Mesh
from jax.sharding import PartitionSpec as P

HEAD = 64
BLOCK = 32
KV = ("z_far", "z_near", "x", "core")
GATHERED = ("z_far", "core")
SELECTED = ("z_near", "x")
FAR_POSITION = 1 << 20
PIECES = 4

VMEM = pl.BlockSpec(memory_space=pltpu.VMEM)
HBM = pl.BlockSpec(memory_space=pltpu.HBM)
SMEM = pl.BlockSpec(memory_space=pltpu.SMEM)
GRANT = pltpu.CompilerParams(vmem_limit_bytes=12 << 20)


def split(number, by):
    return number >> (by.bit_length() - 1), number & (by - 1)


def in_hbm(value):
    return pltpu.with_memory_space_constraint(value, pltpu.HBM)


def prepare_kernel(
    columns,
    cores,
    choice_hbm,
    tokens_hbm,
    key_hbm,
    value_hbm,
    query_hbm,
    slope_hbm,
    listed_hbm,
    rank_ref,
    packed_ref,
    queries_ref,
    choice_ref,
    slope_ref,
    listed_ref,
    place_ref,
    tokens_ref,
    packed_weight_ref,
    query_weight_ref,
    sems,
):
    get_choice, get_slope, put_rank, put_listed = (
        pltpu.make_async_copy(source, target, sems.at[k])
        for k, (source, target) in enumerate(
            (
                (choice_hbm, choice_ref),
                (slope_hbm, slope_ref),
                (place_ref, rank_ref),
                (listed_ref, listed_hbm),
            )
        )
    )
    depth = tokens_ref.shape[1] // PIECES
    pieces = []
    for k in range(PIECES):
        cols = pl.ds(k * depth, depth)
        parts = ()
        if k == 0:
            parts = (
                (key_hbm, packed_weight_ref.at[pl.ds(0, HEAD)]),
                (value_hbm, packed_weight_ref.at[pl.ds(HEAD, HEAD)]),
            )
        parts += (
            (tokens_hbm.at[:, cols], tokens_ref.at[:, cols]),
            (query_hbm.at[cols], query_weight_ref.at[cols]),
        )
        pieces.append(
            [
                pltpu.make_async_copy(source, target, sems.at[4 + 4 * k + n])
                for n, (source, target) in enumerate(parts)
            ]
        )
    get_choice.start()
    for piece in pieces:
        for copy in piece:
            copy.start()
    get_slope.start()
    get_choice.wait()
    blocks_here, topk = choice_ref.shape
    members = lax.axis_size(GATHERED)
    shape = (columns, rank_ref.shape[2])
    column = lax.broadcasted_iota(jnp.int32, shape, 0)
    member = lax.broadcasted_iota(jnp.int32, shape, 1)
    far, core = split(member, cores)
    owner = far * (columns * cores) + column * cores + core
    device, _ = split(choice_ref[0, 0], blocks_here)
    far_owner = (member < members) & (column != split(split(device, cores)[0], columns)[1])
    wanted = jnp.full(shape, -1, jnp.int32)
    for g in range(blocks_here):
        for n in range(1, topk):
            named, local = split(choice_ref[g, n], blocks_here)
            wanted = jnp.where(owner == named, local, wanted)
    wanted = jnp.where(far_owner, wanted, -1)
    needed = wanted >= 0
    upto = needed.astype(jnp.int32)
    step = 1
    while step < members:
        upto = upto + jnp.where(member >= step, pltpu.roll(upto, step, 1), 0)
        step *= 2
    rank = jnp.where(needed, upto - 1, members)
    row = member * blocks_here + wanted
    listed = jnp.full(shape, jnp.max(upto), jnp.int32)
    for place in range(members):
        found = jnp.sum(jnp.where(rank == place, row, 0), axis=1, keepdims=True)
        listed = jnp.where(member == place, found, listed)
    listed_ref[...] = listed.reshape(listed_ref.shape)
    place_ref[...] = rank.reshape(rank_ref.shape)
    put_rank.start()
    put_listed.start()
    packed = queries = 0.0
    for k, piece in enumerate(pieces):
        for copy in piece:
            copy.wait()
        cols = pl.ds(k * depth, depth)
        packed += lax.dot_general(
            tokens_ref[:, cols],
            packed_weight_ref[:, cols],
            (((1,), (1,)), ((), ())),
            preferred_element_type=jnp.float32,
        )
        queries += jnp.dot(
            tokens_ref[:, cols], query_weight_ref[cols], preferred_element_type=jnp.float32
        )
    packed_ref[...] = packed.astype(packed_ref.dtype)
    queries_ref[...] = queries.astype(queries_ref.dtype)
    for copy in (get_slope, put_rank, put_listed):
        copy.wait()


def select_kernel(listed_ref, gathered_ref, outgoing_ref, over_ref):
    columns, places = outgoing_ref.shape[:2]
    longest = listed_ref[0, 0, listed_ref.shape[2] - 1]
    for column in range(1, columns):
        longest = jnp.maximum(longest, listed_ref[column, 0, listed_ref.shape[2] - 1])
    over_ref[0] = (longest > places).astype(jnp.int32)

    for column in range(columns):
        blocks = [gathered_ref[listed_ref[column, 0, place]] for place in range(places)]
        for place, block in enumerate(blocks):
            outgoing_ref[column, place] = block


def attend_kernel(
    cores, choice_ref, slope_ref, rank_ref, queries_ref, gathered_ref, incoming_ref, out_ref
):
    blocks_here, topk = choice_ref.shape
    columns, places = incoming_ref.shape[:2]
    heads = queries_ref.shape[1] // HEAD
    keys = topk * BLOCK
    device, _ = split(choice_ref[0, 0], blocks_here)
    own_column = split(split(device, cores)[0], columns)[1]
    lane = lax.broadcasted_iota(jnp.int32, (BLOCK, 2 * HEAD), 1)
    query_row = lax.broadcasted_iota(jnp.int32, (BLOCK, keys), 0)
    key_lane = lax.broadcasted_iota(jnp.int32, (1, keys), 1)
    tables, raws, fars = [], [], []
    for g in range(blocks_here):
        picked = []
        key_pos = jnp.zeros((1, keys), jnp.int32)
        for n in range(topk):
            chosen = choice_ref[g, n]
            safe = jnp.maximum(chosen, 0)
            owner, local = split(safe, blocks_here)
            chip, core = split(owner, cores)
            far, column = split(chip, columns)
            member = far * cores + core
            here = column == own_column
            place = jnp.minimum(rank_ref[column, 0, member], places - 1)
            row = jnp.where(here, member * blocks_here + local, 0)
            block = jnp.where(here, gathered_ref[row], incoming_ref[column, place])
            picked.append(block)
            first = jnp.where(chosen >= 0, chosen * BLOCK, FAR_POSITION)
            key_pos = jnp.where(split(key_lane, BLOCK)[0] == n, first, key_pos)
        table = jnp.concatenate(picked, axis=0)
        key_pos = key_pos + split(key_lane, BLOCK)[1]
        query_pos = (device * blocks_here + g) * BLOCK + query_row
        distance = query_pos - key_pos
        fars.append(jnp.where(distance >= 0, distance.astype(jnp.float32), jnp.inf))
        rows = pl.ds(g * BLOCK, BLOCK)
        padded = []
        for h in range(heads):
            pair = queries_ref[rows, pl.ds(h // 2 * 2 * HEAD, 2 * HEAD)].astype(jnp.float32)
            if h % 2:
                pair = pltpu.roll(pair, HEAD, 1)
            padded.append(jnp.where(lane < HEAD, pair, 0.0).astype(jnp.bfloat16))
        query = jnp.concatenate(padded, axis=0)
        raws.append(
            lax.dot_general(
                query, table, (((1,), (1,)), ((), ())), preferred_element_type=jnp.float32
            )
        )
        tables.append(table)
    sums = []
    for table, raw, far in zip(tables, raws, fars):
        weights = []
        for h in range(heads):
            scores = raw[h * BLOCK : (h + 1) * BLOCK] * (HEAD**-0.5) - slope_ref[h] * far
            top = jnp.max(scores, axis=1, keepdims=True)
            expd = jnp.exp(scores - top)
            total = jnp.sum(expd, axis=1, keepdims=True)
            weights.append((expd / total).astype(jnp.bfloat16))
        sums.append(
            jnp.dot(jnp.concatenate(weights, axis=0), table, preferred_element_type=jnp.float32)
        )
    for g, summed in enumerate(sums):
        rows = pl.ds(g * BLOCK, BLOCK)
        for h in range(0, heads, 2):
            even = pltpu.roll(summed[h * BLOCK : (h + 1) * BLOCK], HEAD, 1)
            odd = summed[(h + 1) * BLOCK : (h + 2) * BLOCK]
            both = jnp.where(lane < HEAD, even, odd).astype(out_ref.dtype)
            for peer in range(out_ref.shape[0]):
                out_ref[peer, h // 2, rows] = both


def mix_kernel(attended_ref, weight_ref, mixed_hbm, mixed_ref, sems):
    peers, pairs = attended_ref.shape[:2]
    width = mixed_ref.shape[2]
    attended = jnp.concatenate(
        [attended_ref[p, i] for p in range(peers) for i in range(pairs)], axis=1
    )
    copies = []
    for half in range(2):
        cols = pl.ds(half * width, width)
        mixed = jnp.dot(attended, weight_ref[:, cols], preferred_element_type=jnp.float32)
        mixed_ref[half] = mixed.astype(mixed_ref.dtype)
        copies.append(pltpu.make_async_copy(mixed_ref.at[half], mixed_hbm.at[:, cols], sems.at[half]))
        copies[half].start()
    for copy in copies:
        copy.wait()


def shards(tokens, query_weight, key_weight, value_weight, out_weight, alibi_slope, block_choice):
    rows = tokens.shape[0]
    blocks_here = rows // BLOCK
    columns = lax.axis_size(SELECTED)
    cores = lax.axis_size("core")
    members = lax.axis_size(GATHERED)
    peers = lax.axis_size("tp")
    listed, rank, packed, queries, choice, slope = pl.pallas_call(
        functools.partial(prepare_kernel, columns, cores),
        out_shape=(
            jax.ShapeDtypeStruct((columns, 1, 128), jnp.int32),
            pltpu.SMEM((columns, 1, 128), jnp.int32),
            jax.ShapeDtypeStruct((rows, 2 * HEAD), jnp.bfloat16),
            jax.ShapeDtypeStruct((rows, query_weight.shape[1]), jnp.bfloat16),
            pltpu.SMEM(block_choice.shape, jnp.int32),
            pltpu.SMEM(alibi_slope.shape, jnp.float32),
        ),
        in_specs=[HBM] * 6,
        out_specs=(HBM, SMEM, VMEM, VMEM, SMEM, SMEM),
        scratch_shapes=[
            pltpu.VMEM((columns, 1, 128), jnp.int32),
            pltpu.VMEM((columns, 1, 128), jnp.int32),
            pltpu.VMEM(tokens.shape, jnp.bfloat16),
            pltpu.VMEM((2 * HEAD, tokens.shape[1]), jnp.bfloat16),
            pltpu.VMEM(query_weight.shape, jnp.bfloat16),
            pltpu.SemaphoreType.DMA((4 + 4 * PIECES,)),
        ],
        name="prepare",
        compiler_params=GRANT,
    )(
        in_hbm(block_choice),
        in_hbm(tokens),
        in_hbm(key_weight.T),
        in_hbm(value_weight.T),
        in_hbm(query_weight),
        in_hbm(alibi_slope),
    )
    asked = lax.all_to_all(listed, SELECTED, 0, 0, tiled=True)
    gathered = lax.all_gather(packed, GATHERED, axis=0, tiled=True)
    gathered = gathered.reshape(members * blocks_here, BLOCK, 2 * HEAD)
    def select(places, asked, gathered):
        return pl.pallas_call(
            select_kernel,
            out_shape=(
                jax.ShapeDtypeStruct((columns, places, BLOCK, 2 * HEAD), jnp.bfloat16),
                pltpu.SMEM((1,), jnp.int32),
            ),
            in_specs=[SMEM, VMEM],
            out_specs=(VMEM, SMEM),
            name="select",
            compiler_params=GRANT,
        )(asked, gathered)

    def attend(outgoing, choice, slope, rank, queries, gathered):
        incoming = lax.all_to_all(outgoing, SELECTED, 0, 0, tiled=True)
        return pl.pallas_call(
            functools.partial(attend_kernel, cores),
            out_shape=jax.ShapeDtypeStruct(
                (peers, queries.shape[1] // (2 * HEAD), rows, 2 * HEAD), jnp.bfloat16
            ),
            in_specs=[SMEM, SMEM, SMEM, VMEM, VMEM, VMEM],
            out_specs=VMEM,
            name="attend",
            compiler_params=GRANT,
        )(choice, slope, rank, queries, gathered, incoming)

    def short_lists(asked, outgoing, *others):
        return attend(outgoing, *others)

    def long_lists(asked, outgoing, *others):
        outgoing, _ = select(members, asked, others[-1])
        return attend(outgoing, *others)

    outgoing, over = select(block_choice.shape[1] - 1, asked, gathered)
    attended = lax.switch(
        over[0],
        (short_lists, long_lists),
        asked,
        outgoing,
        choice,
        slope,
        rank,
        queries,
        gathered,
    )
    everyone = lax.all_to_all(attended, "tp", 0, 0, tiled=True)
    width = out_weight.shape[1]
    return pl.pallas_call(
        mix_kernel,
        out_shape=jax.ShapeDtypeStruct((rows, width), jnp.bfloat16),
        in_specs=[VMEM, VMEM],
        out_specs=HBM,
        scratch_shapes=[
            pltpu.VMEM((2, rows, width // 2), jnp.bfloat16),
            pltpu.SemaphoreType.DMA((2,)),
        ],
        name="mix",
        compiler_params=GRANT,
    )(everyone, out_weight)


def solution(mesh):
    split = Mesh(
        mesh.devices.reshape(8, 2, 4, 2, mesh.shape["tp"]), ("z_far", "z_near", "x", "core", "tp")
    )
    placed = (
        P(KV, None),
        P(None, "tp"),
        P(None, "tp"),
        P(None, "tp"),
        P(None, "tp"),
        P("tp"),
        P(KV, None),
    )
    return jax.shard_map(
        shards, mesh=split, in_specs=placed, out_specs=P(KV, "tp"), check_vma=False
    )
```
